512 devices in a mesh: ep: 32 (over z, x), tp: 16 (over y, core).
Axes of the slice: x: 4, y: 8, z: 8, core: 2. Of those that a mesh axis runs over, the one named last changes fastest.
Arguments:
- query_rows: bfloat16 [12288, 4096], P('ep', 'tp'), may hold values from -6 to 6
- key_rows: bfloat16 [12288, 2048], P('ep', 'tp'), may hold values from -6 to 6
- value_rows: bfloat16 [12288, 2048], P('ep', 'tp'), may hold values from -6 to 6
- query_gain: float32 [128], replicated, may hold values from 0.4 to 5
- key_gain: float32 [128], replicated, may hold values from 0.4 to 5
- w_out: bfloat16 [4096, 2048], P('tp'), may hold values from -0.09375 to 0.09375
- mixer_gain: float32 [2048], replicated, may hold values from 0.1 to 1.9
- expert_input: bfloat16 [6144, 2048], P('ep'), may hold values from -6 to 6
- expert_ids: int32 [6144, 2], P('ep'), may hold values from 0 to 31, as said below
- expert_weights: float32 [6144, 2], P('ep'), may hold values from 0.1 to 1
- input_gain: float32 [2048], replicated, may hold values from 0.1 to 1.9
- w_gate: bfloat16 [32, 2048, 4096], P('ep', None, 'tp'), may hold values from -0.125 to 0.125
- w_up: bfloat16 [32, 2048, 4096], P('ep', None, 'tp'), may hold values from -0.125 to 0.125
- w_down: bfloat16 [32, 4096, 2048], P('ep', 'tp'), may hold values from -2 to 2
- out_gain: float32 [2048], P('tp'), may hold values from 0.1 to 1.9
Outputs:
- mixer_result: bfloat16 [12288, 2048], P(('ep', 'tp'))
- moe_result: bfloat16 [6144, 2048], P('ep', 'tp')
The draws below stay inside these ranges and needn't reach their ends.
Inputs may be any that keep to these rules, and one draw needn't show every extreme that they name: `expert_ids`: the two experts of a row differ and lie in one group of 8 consecutive experts. Among the rows of one index of ep (aligned blocks of 192 rows) no expert is named by more than 18 rows, and in every block some expert is named by exactly 18 rows.
All inputs are finite; a program needn't handle non-finite values.
Results may differ from the reference program's by a relative error of at most 0.02.
The reference program's roundings to bfloat16 on the way count: a program that leaves them out, or rounds other values in their place, can miss the bound.
Values may be sent and summed in bfloat16 or wider, within the bound.
A program may use at most 64 MiB of HBM per device.

```python
import math
import jax
import jax.numpy as jnp
from jax import lax

D = 2048
HEADS = 32
KV_HEADS = 16
HEAD = 128
GRID = 64
FF = 4096
GROUPS = 4
TOP = 2
ROWS2 = 192
EXPERTS = 32
INNER = 8
CAP = 18
TOK1 = 12288
TOK2 = 6144
N_EP = 32
N_TP = 16


def key_field(key):
    normal_base = jax.random.normal(jax.random.fold_in(key, 11), (TOK1, KV_HEADS * HEAD), jnp.float32)
    return jnp.clip(normal_base, -6.0, 6.0)


def draw_key_rows(key, part):
    return key_field(key).astype(jnp.bfloat16)


def draw_query_rows(key, part):
    fresh = jax.random.normal(jax.random.fold_in(key, 12), (TOK1, HEADS * HEAD), jnp.float32)
    return jnp.clip(fresh, -6.0, 6.0).astype(jnp.bfloat16)


def gain_field(key, offset):
    return jax.random.uniform(jax.random.fold_in(key, offset), (HEAD,), jnp.float32, 0.4, 1.6)


def draw_query_gain(key, part):
    return gain_field(key, 31)


def draw_key_gain(key, part):
    return gain_field(key, 32)


def draw_w_down(key, part):
    normal_base = jax.random.normal(jax.random.fold_in(key, 21), (EXPERTS, FF, D), jnp.float32) * FF ** (-0.5)
    column_ramp = jnp.exp(2.3 * jnp.arange(D, dtype=jnp.float32) / D)
    jitter = jax.random.uniform(jax.random.fold_in(key, 22), (D,), jnp.float32, 0.5, 1.5)
    return jnp.clip(normal_base * column_ramp * jitter, -2.0, 2.0).astype(jnp.bfloat16)


def block_ids(block_key):
    eighth = ROWS2 // 8
    shares = jnp.array([1, 2, 2, 3], jnp.int32)[jax.random.permutation(jax.random.fold_in(block_key, 1), 4)]
    group_sizes = shares * eighth
    group_ends = jnp.cumsum(group_sizes)
    starts = group_ends - group_sizes
    row_order = jnp.arange(ROWS2, dtype=jnp.int32)
    group_of = jnp.sum((row_order[:, None] >= group_ends[None, :]).astype(jnp.int32), axis=1)
    within = row_order - starts[group_of]
    shifts = jax.random.randint(jax.random.fold_in(block_key, 2), (GROUPS,), 1, INNER)
    labels = jax.vmap(lambda offset: jax.random.permutation(jax.random.fold_in(block_key, offset), INNER))(jnp.arange(GROUPS) + 3)
    first_pick = labels[group_of, within % INNER]
    second_pick = labels[group_of, (within + shifts[group_of]) % INNER]
    chosen_ids = jnp.stack([first_pick, second_pick], axis=1) + INNER * group_of[:, None]
    shuffle = jax.random.permutation(jax.random.fold_in(block_key, 9), ROWS2)
    return chosen_ids[shuffle].astype(jnp.int32)


def draw_expert_ids(key, part):
    block_keys = jax.vmap(lambda block_index: jax.random.fold_in(key, block_index))(jnp.arange(N_EP) + 100)
    return jax.vmap(block_ids)(block_keys).reshape(TOK2, TOP)


def shard_levels(own_key, dims, shards, smallest, top_value):
    loudness, own = 1.0, jax.random.fold_in(own_key, 6)
    for dim, parts in shards:
        steps = jnp.exp(jax.random.uniform(jax.random.fold_in(own, dim), (parts,), jnp.float32, smallest / len(shards), top_value / len(shards)))
        loudness = loudness * jnp.repeat(steps, dims[dim] // parts).reshape([-1 if axis == dim else 1 for axis in range(len(dims))])
    return loudness


def scatter_about(rng, dims, width, reach, pieces=(), held_as=jnp.bfloat16):
    level = shard_levels(rng, dims, pieces, -0.22, 0.18) if pieces else 1.0
    drawn = jax.random.normal(rng, dims, jnp.float32) * width * level
    return jnp.minimum(jnp.maximum(drawn, -reach), reach).astype(held_as)


def setup_inputs(seed: int = 0) -> dict:
    key_list = jax.random.split(jax.random.key(seed), 16)
    query_rows = draw_query_rows(jax.random.fold_in(key_list[15], 71), 0)
    key_rows = draw_key_rows(jax.random.fold_in(key_list[15], 71), 0)
    value_rows = scatter_about(key_list[2], (TOK1, KV_HEADS * HEAD), 1.0, 6.0, ((0, 32), (1, 16)))
    query_gain = draw_query_gain(jax.random.fold_in(key_list[15], 71), 0)
    key_gain = draw_key_gain(jax.random.fold_in(key_list[15], 71), 0)
    w_out = scatter_about(key_list[5], (HEADS * HEAD, D), (HEADS * HEAD) ** -0.5, 0.09375, ((0, 16),))
    mixer_gain = jnp.clip(1.0 + 0.18 * jax.random.normal(key_list[6], (D,), jnp.float32), 0.1, 1.9)
    expert_input = scatter_about(key_list[7], (TOK2, D), 1.0, 6.0, ((0, 32),))
    expert_ids = draw_expert_ids(jax.random.fold_in(key_list[15], 71), 0)
    expert_weights = jnp.clip(jnp.exp(math.log(1.0) - 2.3025851 * jax.random.uniform(key_list[9], (TOK2, TOP), jnp.float32) ** shard_levels(key_list[9], (TOK2, TOP), ((0, 32),), -0.2, 0.2)), 0.1, 1.0)
    input_gain = jnp.clip(1.0 + 0.18 * jax.random.normal(key_list[10], (D,), jnp.float32), 0.1, 1.9)
    w_gate = scatter_about(key_list[11], (EXPERTS, D, FF), D ** -0.5, 0.125, ((0, 32), (2, 16)))
    w_up = scatter_about(key_list[12], (EXPERTS, D, FF), D ** -0.5, 0.125, ((0, 32), (2, 16)))
    w_down = draw_w_down(jax.random.fold_in(key_list[15], 71), 0)
    out_gain = jnp.clip(1.0 + 0.18 * jax.random.normal(key_list[14], (D,), jnp.float32), 0.1, 1.9)
    return {"query_rows": query_rows, "key_rows": key_rows, "value_rows": value_rows, "query_gain": query_gain, "key_gain": key_gain, "w_out": w_out, "mixer_gain": mixer_gain, "expert_input": expert_input, "expert_ids": expert_ids, "expert_weights": expert_weights, "input_gain": input_gain, "w_gate": w_gate, "w_up": w_up, "w_down": w_down, "out_gain": out_gain}


EPS = 1e-06
THETA = 10000.0

def turn_half(half_part, position):
    half_width = half_part.shape[-1]
    frequency = THETA ** (-jnp.arange(0, half_width, 2, dtype=jnp.float32) / half_width)
    angles = position[:, None, None] * frequency[None, None, :]
    cosine = jnp.cos(angles)
    sine_part = jnp.sin(angles)
    first_half = half_part[..., :half_width // 2]
    second = half_part[..., half_width // 2:]
    return jnp.concatenate([first_half * cosine - second * sine_part, second * cosine + first_half * sine_part], axis=-1)

def norm_turn(raw_rows, gain_vec, row_offset):
    row_count = raw_rows.shape[0]
    head_dim = gain_vec.shape[0]
    head_count = raw_rows.shape[1] // head_dim
    by_head = raw_rows.astype(jnp.float32).reshape(row_count, head_count, head_dim)
    scaled = by_head * lax.rsqrt(lax.optimization_barrier(jnp.mean(by_head * by_head, axis=-1, keepdims=True)) + EPS) * gain_vec
    position = row_offset + jnp.arange(row_count, dtype=jnp.int32)
    grid_row = (position // GRID).astype(jnp.float32)
    grid_col = (position % GRID).astype(jnp.float32)
    half_dim = head_dim // 2
    turned = jnp.concatenate([turn_half(scaled[..., :half_dim], grid_row), turn_half(scaled[..., half_dim:], grid_col)], axis=-1)
    return turned.reshape(row_count, head_count * head_dim).astype(jnp.bfloat16)

def mixer_ref(query_rows, key_rows, value_rows, query_gain, key_gain, w_out, mixer_gain):
    token_count = query_rows.shape[0]
    group_size = HEADS // KV_HEADS
    query_turned = norm_turn(query_rows, query_gain, 0)
    key_turned = norm_turn(key_rows, key_gain, 0)
    query_heads = query_turned.reshape(token_count, HEADS, HEAD).transpose(1, 0, 2)
    key_heads = jnp.repeat(key_turned.reshape(token_count, KV_HEADS, HEAD).transpose(1, 0, 2), group_size, axis=0)
    value_heads = jnp.repeat(value_rows.reshape(token_count, KV_HEADS, HEAD).transpose(1, 0, 2), group_size, axis=0)

    def one_head(head_triple):
        query_head, key_head, value_head = head_triple
        scores = jnp.dot(query_head, key_head.T, preferred_element_type=jnp.float32) * HEAD ** (-0.5)
        row_max = lax.optimization_barrier(jnp.max(scores, axis=1, keepdims=True))
        exponent = jnp.exp(scores - row_max)
        probs = exponent.astype(jnp.bfloat16)
        numer = jnp.dot(probs, value_head, preferred_element_type=jnp.float32)
        return (numer / lax.optimization_barrier(jnp.sum(exponent, axis=1, keepdims=True))).astype(jnp.bfloat16)
    attended = lax.map(one_head, (query_heads, key_heads, value_heads))
    attended = attended.transpose(1, 0, 2).reshape(token_count, HEADS * HEAD)
    block_width = HEADS * HEAD // N_TP
    attended_blocks = attended.reshape(token_count, N_TP, block_width).transpose(1, 0, 2)
    weight_blocks = w_out.reshape(N_TP, block_width, D)

    def add_part(running_sum, block_pair):
        attended_block, weight_block = block_pair
        head_part = jnp.dot(attended_block, weight_block, preferred_element_type=jnp.float32).astype(jnp.bfloat16)
        head_part = lax.optimization_barrier(head_part)
        return (running_sum + head_part.astype(jnp.float32), None)
    mixed_sum, _ = lax.scan(add_part, jnp.zeros((token_count, D), jnp.float32), (attended_blocks, weight_blocks))
    scaled = mixed_sum * lax.rsqrt(lax.optimization_barrier(jnp.mean(mixed_sum * mixed_sum, axis=1, keepdims=True)) + EPS) * mixer_gain
    return scaled.astype(jnp.bfloat16)

def expert_ref(expert_input, expert_ids, expert_weights, input_gain, w_gate, w_up, w_down, out_gain):
    token_count = expert_input.shape[0]
    inputs_f = expert_input.astype(jnp.float32)
    normed = (inputs_f * lax.rsqrt(lax.optimization_barrier(jnp.mean(inputs_f * inputs_f, axis=1, keepdims=True)) + EPS) * input_gain).astype(jnp.bfloat16)
    padded = jnp.concatenate([normed, jnp.zeros((1, D), jnp.bfloat16)], axis=0)
    flat_ids = expert_ids.reshape(-1)
    pick_count = flat_ids.shape[0]
    top_count = expert_ids.shape[1]
    weight_flat = jnp.concatenate([expert_weights.reshape(-1), jnp.zeros((1,), jnp.float32)])
    slot_total = N_EP * CAP
    block_width = FF // N_TP

    def one_expert(accum, expert_index):
        chosen = flat_ids == expert_index
        position = jnp.cumsum(chosen.astype(jnp.int32)) - 1
        target = jnp.where(chosen, position, slot_total).astype(jnp.int32)
        pick_table = jnp.full((slot_total,), pick_count, jnp.int32).at[target].set(jnp.arange(pick_count, dtype=jnp.int32), mode='drop')
        token_table = (pick_table // top_count).astype(jnp.int32)
        gathered = jnp.take(padded, token_table, axis=0)
        gate_weight = lax.dynamic_index_in_dim(w_gate, expert_index, 0, keepdims=False)
        up_weight = lax.dynamic_index_in_dim(w_up, expert_index, 0, keepdims=False)
        down_weight = lax.dynamic_index_in_dim(w_down, expert_index, 0, keepdims=False)
        gate_pre = jnp.dot(gathered, gate_weight, preferred_element_type=jnp.float32)
        up_pre = jnp.dot(gathered, up_weight, preferred_element_type=jnp.float32)
        hidden = (jax.nn.silu(gate_pre) * up_pre).astype(jnp.bfloat16)
        hidden_blocks = hidden.reshape(slot_total, N_TP, block_width).transpose(1, 0, 2).astype(jnp.float32)
        down_blocks = down_weight.reshape(N_TP, block_width, D).astype(jnp.float32)
        expert_part = jnp.einsum('jsf,jfd->jsd', hidden_blocks, down_blocks).astype(jnp.bfloat16)
        expert_part = lax.optimization_barrier(expert_part)
        expert_rows = lax.optimization_barrier(jnp.sum(expert_part.astype(jnp.float32), axis=0)).astype(jnp.bfloat16)
        weights_now = jnp.take(weight_flat, pick_table)
        accum = accum.at[token_table].add(weights_now[:, None] * expert_rows.astype(jnp.float32), mode='drop')
        return (accum, None)
    combined, _ = lax.scan(one_expert, jnp.zeros((token_count, D), jnp.float32), jnp.arange(EXPERTS, dtype=jnp.int32))
    scaled = combined * lax.rsqrt(lax.optimization_barrier(jnp.mean(combined * combined, axis=1, keepdims=True)) + EPS) * out_gain
    return scaled.astype(jnp.bfloat16)

def reference(query_rows, key_rows, value_rows, query_gain, key_gain, w_out, mixer_gain, expert_input, expert_ids, expert_weights, input_gain, w_gate, w_up, w_down, out_gain):
    mixer_result = mixer_ref(query_rows, key_rows, value_rows, query_gain, key_gain, w_out, mixer_gain)
    moe_result = expert_ref(expert_input, expert_ids, expert_weights, input_gain, w_gate, w_up, w_down, out_gain)
    return (mixer_result, moe_result)
```

```python
import functools
from types import SimpleNamespace

import numpy as np
import jax
import jax.numpy as jnp
from jax import lax
from jax.experimental import pallas as pl
from jax.experimental.pallas import tpu as pltpu
from jax.sharding import Mesh
from jax.sharding import PartitionSpec as P

NZ, NX, NY, NC = 8, 4, 8, 2
EP = ("z", "x")
TP = ("y", "c")
D = 2048
HEAD = 128
GRID = 64
ROWS = 384
TOKENS2 = 192
CAP = 18
SLAB = 32
EXPERTS = 32
SLOTS = EXPERTS * CAP
PADDED = EXPERTS * SLAB
EPS = 1e-06
THETA = 10000.0
F32 = jnp.float32
BF16 = jnp.bfloat16
MESH_ID = pl.DeviceIdType.MESH
FAR_FIRST = (4, 3, 5, 2, 6, 1, 7, 0)
X_ORDER = (2, 1, 3, 0)


def around(i, d, n):
    return lax.rem(i + (d % n), n)


def here():
    a = SimpleNamespace()
    a.z, a.x, a.y, a.c = (lax.axis_index(n) for n in ("z", "x", "y", "c"))
    a.ep = a.z * NX + a.x
    return a


def remote(src, dst, ss, rs, **dev):
    return pltpu.make_async_remote_copy(
        src_ref=src, dst_ref=dst, send_sem=ss, recv_sem=rs, device_id=dev, device_id_type=MESH_ID
    )


def ep_peer(a, k):
    e = lax.rem(a.ep + k, EXPERTS)
    return e, lax.div(e, NX), lax.rem(e, NX)


def greet_ep(a, barrier):
    def one(k, carry):
        _, z, x = ep_peer(a, k)
        pl.semaphore_signal(barrier, inc=1, device_id={"z": z, "x": x}, device_id_type=MESH_ID)
        return carry

    lax.fori_loop(1, EXPERTS, one, 0)


def greet_tp(a, barrier, cores):
    for d in range(NY):
        for o in range(cores):
            if d or o:
                c = a.c if o == 0 else 1 - a.c
                pl.semaphore_signal(
                    barrier, inc=1, device_id={"y": around(a.y, d, NY), "c": c}, device_id_type=MESH_ID
                )


def wait_bytes(ref, sem):
    pltpu.make_async_copy(ref, ref, sem).wait()


def iota(shape, dim):
    return lax.broadcasted_iota(jnp.int32, shape, dim)


def eye128():
    return iota((128, 128), 0) == iota((128, 128), 1)


def to_row(col):
    return jnp.sum(jnp.where(eye128(), col, 0.0), axis=0, keepdims=True)


def to_col(row):
    return jnp.sum(jnp.where(eye128(), row, 0.0), axis=1, keepdims=True)


MOE_IN = ("xin", "srow", "scol", "wts", "igain", "ogain", "wg_h", "wu_h", "wd_h")
MOE_SCRATCH = dict(
    disp=pltpu.VMEM((EXPERTS, SLAB, 256), BF16),
    drecv=pltpu.VMEM((EXPERTS, SLAB, 256), BF16),
    xg=pltpu.VMEM((2, 4, 2, SLOTS, 128), BF16),
    xcat=pltpu.VMEM((SLOTS, D), BF16),
    wg=pltpu.VMEM((D, 256), BF16),
    wu=pltpu.VMEM((D, 256), BF16),
    wd=pltpu.VMEM((256, D), BF16),
    part=pltpu.VMEM((2, NY, SLOTS, 128), BF16),
    pr=pltpu.VMEM((NY, SLOTS, 128), BF16),
    ps=pltpu.VMEM((NY, SLOTS, 128), BF16),
    own=pltpu.VMEM((SLOTS, 128), F32),
    rs=pltpu.VMEM((NY, SLOTS, 128), BF16),
    rsend=pltpu.VMEM((EXPERTS, SLAB, 128), BF16),
    rrecv=pltpu.VMEM((EXPERTS, SLAB, 128), BF16),
    comb=pltpu.VMEM((TOKENS2, 128), F32),
    sqs=pltpu.VMEM((8, 128), F32),
    sqr=pltpu.VMEM((16, 8, 128), F32),
    w_sem=pltpu.SemaphoreType.DMA((3,)),
    d_ss=pltpu.SemaphoreType.DMA,
    d_rs=pltpu.SemaphoreType.DMA,
    ag_ss=pltpu.SemaphoreType.DMA((3,)),
    ag_rs=pltpu.SemaphoreType.DMA((3,)),
    pf_ss=pltpu.SemaphoreType.DMA((4,)),
    pf_rs=pltpu.SemaphoreType.DMA((4,)),
    pp_ss=pltpu.SemaphoreType.DMA((8,)),
    pp_rs=pltpu.SemaphoreType.DMA((8,)),
    rs_ss=pltpu.SemaphoreType.DMA((8,)),
    rs_rs=pltpu.SemaphoreType.DMA((8,)),
    t_ss=pltpu.SemaphoreType.DMA,
    t_rs=pltpu.SemaphoreType.DMA,
    q_ss=pltpu.SemaphoreType.DMA,
    q_rs=pltpu.SemaphoreType.DMA,
)


def moe_weights(r):
    for i, (src, dst) in enumerate(((r.wg_h, r.wg), (r.wu_h, r.wu), (r.wd_h, r.wd))):
        pltpu.make_async_copy(src, dst, r.w_sem.at[i]).start()


def moe_weights_wait(r):
    for i, (src, dst) in enumerate(((r.wg_h, r.wg), (r.wu_h, r.wu), (r.wd_h, r.wd))):
        pltpu.make_async_copy(src, dst, r.w_sem.at[i]).wait()


def moe_dispatch_build(a, r):
    x = r.xin[...].astype(F32)
    inv = lax.rsqrt(jnp.sum(x * x, axis=1, keepdims=True) * (1.0 / D) + EPS)
    g = lax.rem(a.y, 4)
    halves = []
    for j in range(2):
        off = pl.multiple_of(((g + 4 * j) * 2 + a.c) * 128, 128)
        xs = r.xin[:, pl.ds(off, 128)].astype(F32)
        halves.append((xs * inv * r.igain[:, pl.ds(off, 128)]).astype(BF16))
    nn = jnp.concatenate(halves, axis=1)
    rows = iota((PADDED, TOKENS2), 0)
    pick = (rows == r.srow[0:1, :]) | (rows == r.srow[1:2, :])
    pick = jnp.where(pick, 1.0, 0.0).astype(BF16)
    out = jnp.dot(pick, nn, preferred_element_type=F32).astype(BF16)
    r.disp[...] = out.reshape(EXPERTS, SLAB, 256)


def exchange_start(a, src, dst, ss, rs):
    def one(k, carry):
        e, z, x = ep_peer(a, k)
        remote(src.at[e], dst.at[a.ep], ss, rs, z=z, x=x).start()
        return carry

    lax.fori_loop(1, EXPERTS, one, 0)
    dst[a.ep] = src[a.ep]


def exchange_wait(src, dst, ss, rs):
    wait_bytes(dst.at[pl.ds(0, EXPERTS - 1)], rs)
    wait_bytes(src.at[pl.ds(0, EXPERTS - 1)], ss)


def padded_place(i):
    e = ((i.astype(F32) + 0.5) * (1.0 / CAP)).astype(jnp.int32)
    return i + e * (SLAB - CAP)


def moe_compact(a, r):
    g = lax.rem(a.y, 4)
    place = padded_place(iota((SLOTS, 1), 0))
    pick = jnp.where(iota((SLOTS, PADDED), 1) == place, 1.0, 0.0).astype(BF16)
    got = r.drecv[...].reshape(PADDED, 256)
    out = jnp.dot(pick, got, preferred_element_type=F32).astype(BF16)
    r.xg[a.c, g, 0] = out[:, :128]
    r.xg[a.c, g, 1] = out[:, 128:]


def moe_gather_copies(a, r):
    g = lax.rem(a.y, 4)
    src = r.xg.at[a.c, g]
    two = around(a.y, 2, NY) + a.c * 4
    targets = (around(a.y, 1, NY), around(a.y, -1, NY), lax.rem(two, NY))
    return [remote(src, src, r.ag_ss.at[i], r.ag_rs.at[i], y=t) for i, t in enumerate(targets)]


def moe_group(a, i):
    g = lax.rem(a.y, 4)
    return g if i == 0 else around(g, (3, 1, 2)[i - 1], 4)


def moe_partner_copy(a, r, i):
    src = r.xg.at[a.c, moe_group(a, i)]
    return remote(src, src, r.pf_ss.at[i], r.pf_rs.at[i], c=1 - a.c)


def moe_gather_start(a, r):
    for cp in moe_gather_copies(a, r):
        cp.start()
    moe_partner_copy(a, r, 0).start()


def moe_gather_forward(a, r, i):
    moe_gather_copies(a, r)[i - 1].wait_recv()
    moe_partner_copy(a, r, i).start()


def moe_gather_finish(a, r):
    for cp in moe_gather_copies(a, r):
        cp.wait_send()
    for i in range(4):
        moe_partner_copy(a, r, i).wait()


def moe_experts(a, r):
    for par in range(2):
        for g in range(4):
            for h in range(2):
                at = ((g + 4 * h) * 2 + par) * 128
                r.xcat[:, at : at + 128] = r.xg[par, g, h]
    moe_weights_wait(r)

    def block(b, carry):
        at = pl.ds(pl.multiple_of(b * 192, 192), 192)
        xb = r.xcat[at, :]
        gate = jnp.dot(xb, r.wg[...], preferred_element_type=F32)
        up = jnp.dot(xb, r.wu[...], preferred_element_type=F32)
        hid = (gate / (1.0 + jnp.exp(-gate)) * up).astype(BF16)
        for ys in range(NY):
            o = jnp.dot(hid, r.wd[:, ys * 256 : ys * 256 + 256], preferred_element_type=F32)
            o = o.astype(BF16)
            r.part[0, ys, at, :] = o[:, :128]
            r.part[1, ys, at, :] = o[:, 128:]
        return carry

    lax.fori_loop(0, SLOTS // 192, block, 0)


def moe_pair_copy(a, r, i):
    ys = around(a.y, FAR_FIRST[i], NY)
    return remote(r.part.at[1 - a.c, ys], r.pr.at[ys], r.pp_ss.at[i], r.pp_rs.at[i], c=1 - a.c)


def moe_sum_copy(a, r, d):
    ys = around(a.y, d, NY)
    return remote(r.ps.at[ys], r.rs.at[d], r.rs_ss.at[d], r.rs_rs.at[d], y=ys)


def moe_pair_start(a, r):
    for i in range(NY):
        moe_pair_copy(a, r, i).start()


def moe_pair_sum(a, r, i):
    d = FAR_FIRST[i]
    ys = around(a.y, d, NY)
    moe_pair_copy(a, r, i).wait_recv()
    total = r.part[a.c, ys].astype(F32) + r.pr[ys].astype(F32)
    if d:
        r.ps[ys] = total.astype(BF16)
        moe_sum_copy(a, r, d).start()
    else:
        r.own[...] = total


def moe_return_start(a, r):
    total = r.own[...]
    for d in range(1, NY):
        moe_sum_copy(a, r, d).wait_recv()
        total = total + r.rs[d].astype(F32)
    rows = total.astype(BF16)
    place = padded_place(iota((1, SLOTS), 1))
    pick = jnp.where(iota((PADDED, SLOTS), 0) == place, 1.0, 0.0).astype(BF16)
    out = jnp.dot(pick, rows, preferred_element_type=F32).astype(BF16)
    r.rsend[...] = out.reshape(EXPERTS, SLAB, 128)
    exchange_start(a, r.rsend, r.rrecv, r.t_ss, r.t_rs)


def square_targets(a):
    out = []
    for d in range(NY):
        for o in range(2):
            if d or o:
                out.append((around(a.y, d, NY), a.c if o == 0 else 1 - a.c))
    return out


def moe_combine(a, r):
    exchange_wait(r.rsend, r.rrecv, r.t_ss, r.t_rs)
    got = r.rrecv[...].reshape(PADDED, 128)
    total = None
    for k in range(2):
        pick = jnp.where(iota((TOKENS2, PADDED), 1) == r.scol[:, k : k + 1], 1.0, 0.0).astype(BF16)
        term = jnp.dot(pick, got, preferred_element_type=F32) * r.wts[:, k : k + 1]
        total = term if total is None else total + term
    r.comb[...] = total
    sq = jnp.sum(total * total, axis=1, keepdims=True)
    r.sqs[...] = jnp.zeros((8, 128), F32)
    r.sqs[0:1, :] = to_row(sq[:128])
    r.sqs[1:2, :] = to_row(sq[64:])
    tp = a.y * 2 + a.c
    for y, c in square_targets(a):
        remote(r.sqs, r.sqr.at[tp], r.q_ss, r.q_rs, y=y, c=c).start()
    r.sqr[tp] = r.sqs[...]


def moe_finish(a, r, out):
    wait_bytes(r.sqr.at[pl.ds(0, 15)], r.q_rs)
    wait_bytes(r.sqr.at[pl.ds(0, 15)], r.q_ss)
    tot = r.sqr[0]
    for i in range(1, 16):
        tot = tot + r.sqr[i]
    inv = lax.rsqrt(tot * (1.0 / D) + EPS)
    lo, hi = to_col(inv[0:1, :]), to_col(inv[1:2, :])
    out[0:128, :] = (r.comb[0:128, :] * lo * r.ogain[...]).astype(BF16)
    out[128:192, :] = (r.comb[128:192, :] * hi[64:] * r.ogain[...]).astype(BF16)
    for d in range(1, NY):
        moe_sum_copy(a, r, d).wait_send()
    for i in range(NY):
        moe_pair_copy(a, r, i).wait_send()


MIX_IN = ("q_in", "k_in", "v_in", "qg", "kg", "rowcs", "colcs", "mgain", "wo_h")
MIX_SCRATCH = dict(
    q_all=pltpu.VMEM((NX, 2 * ROWS, HEAD), BF16),
    kt=pltpu.VMEM((NZ, HEAD, ROWS), BF16),
    va=pltpu.VMEM((NZ, ROWS, HEAD), BF16),
    kx=pltpu.VMEM((HEAD, 2 * ROWS), BF16),
    vx=pltpu.VMEM((2 * ROWS, 256), BF16),
    mx=pltpu.VMEM((NX, 2 * ROWS, 128), F32),
    acc=pltpu.VMEM((NX, 2 * ROWS, 256), F32),
    ob=pltpu.VMEM((NX, 2 * ROWS, HEAD), BF16),
    lb=pltpu.VMEM((NX, 8, 128), F32),
    orc=pltpu.VMEM((NX, 2 * ROWS, HEAD), BF16),
    lrc=pltpu.VMEM((NX, 8, 128), F32),
    att=pltpu.VMEM((ROWS, 256), BF16),
    wo=pltpu.VMEM((256, D), BF16),
    mp=pltpu.VMEM((2, ROWS, 1024), BF16),
    mr=pltpu.VMEM((ROWS, 1024), BF16),
    ms=pltpu.VMEM((NY, 48, 1024), BF16),
    yr=pltpu.VMEM((NY, 48, 1024), BF16),
    fs=pltpu.VMEM((48, 1024), F32),
    fr=pltpu.VMEM((24, 1024), F32),
    wo_sem=pltpu.SemaphoreType.DMA,
    xq_ss=pltpu.SemaphoreType.DMA((4,)),
    xq_rs=pltpu.SemaphoreType.DMA((4,)),
    k_ss=pltpu.SemaphoreType.DMA((8,)),
    k_rs=pltpu.SemaphoreType.DMA((8,)),
    v_ss=pltpu.SemaphoreType.DMA((8,)),
    v_rs=pltpu.SemaphoreType.DMA((8,)),
    o_ss=pltpu.SemaphoreType.DMA((4,)),
    o_rs=pltpu.SemaphoreType.DMA((4,)),
    l_ss=pltpu.SemaphoreType.DMA((4,)),
    l_rs=pltpu.SemaphoreType.DMA((4,)),
    m_ss=pltpu.SemaphoreType.DMA((2,)),
    m_rs=pltpu.SemaphoreType.DMA((2,)),
    y_ss=pltpu.SemaphoreType.DMA((8,)),
    y_rs=pltpu.SemaphoreType.DMA((8,)),
    f_ss=pltpu.SemaphoreType.DMA,
    f_rs=pltpu.SemaphoreType.DMA,
)
OWN = 7


def swap_parts(v):
    lane = lax.rem(iota(v.shape, 1), 64)
    return jnp.where(lane < 32, pltpu.roll(v, 96, 1), pltpu.roll(v, 32, 1))


def turned(a, r, block, gain, g):
    v = block.astype(F32)
    v = v * lax.rsqrt(jnp.mean(v * v, axis=1, keepdims=True) + EPS) * gain
    at = a.ep * (ROWS // GRID) + g
    cos = r.rowcs[0, pl.ds(at, 1), :] + r.colcs[0]
    sin = r.rowcs[1, pl.ds(at, 1), :] + r.colcs[1]
    return (v * cos + swap_parts(v) * sin).astype(BF16)


def mix_turn(a, r):
    pltpu.make_async_copy(r.wo_h, r.wo, r.wo_sem).start()
    keys = []
    for g in range(ROWS // GRID):
        at = slice(g * GRID, g * GRID + GRID)
        for h in range(2):
            q = turned(a, r, r.q_in[at, h * 128 : h * 128 + 128], r.qg[...], g)
            r.q_all[a.x, h * ROWS + g * GRID : h * ROWS + g * GRID + GRID, :] = q
        keys.append(turned(a, r, r.k_in[at, :], r.kg[...], g))
    key = jnp.concatenate(keys, axis=0)
    r.kt[OWN] = key.astype(F32).T.astype(BF16)
    r.va[OWN] = r.v_in[...]
    r.vx[:, 128:] = jnp.ones((2 * ROWS, 128), BF16)
    r.mx[...] = jnp.full(r.mx.shape, -1e30, F32)
    r.acc[...] = jnp.zeros(r.acc.shape, F32)


def q_copy(a, r, d):
    mine = r.q_all.at[a.x]
    return remote(mine, mine, r.xq_ss.at[d], r.xq_rs.at[d], x=around(a.x, d, NX))


def kv_copies(a, r, slot):
    src = OWN if slot < 2 else slot - 2
    z = around(a.z, 1 if slot % 2 == 0 else -1, NZ)
    return (
        remote(r.kt.at[src], r.kt.at[slot], r.k_ss.at[slot], r.k_rs.at[slot], z=z),
        remote(r.va.at[src], r.va.at[slot], r.v_ss.at[slot], r.v_rs.at[slot], z=z),
    )


def kv_start(a, r, slot):
    for cp in kv_copies(a, r, slot):
        cp.start()


def kv_arrived(a, r, slot):
    for cp in kv_copies(a, r, slot):
        cp.wait_recv()
    if slot + 2 < OWN:
        kv_start(a, r, slot + 2)


def mix_send(a, r):
    kv_start(a, r, 0)
    kv_start(a, r, 1)
    for d in (2, 1, 3):
        q_copy(a, r, d).start()


def attend_rows(r, xs, at):
    q = r.q_all[xs, at, :]
    s = jnp.dot(q, r.kx[...], preferred_element_type=F32)
    old = r.mx[xs, at, :]
    new = jnp.maximum(old, jnp.max(s, axis=1, keepdims=True))
    r.mx[xs, at, :] = new
    p = jnp.concatenate(
        [jnp.exp2(s[:, j * 128 : j * 128 + 128] - new).astype(BF16) for j in range(6)], axis=1
    )
    keep = jnp.exp2(old - new)
    pv = jnp.dot(p, r.vx[...], preferred_element_type=F32)
    acc = r.acc[xs, at, :]
    r.acc[xs, at, :] = acc * jnp.concatenate([keep, keep], axis=1) + pv


TILE = 256


def mix_step(a, r, s):
    slots = (2 * s, 2 * s + 1)
    for slot in slots:
        if slot != OWN:
            kv_arrived(a, r, slot)
    for i, slot in enumerate(slots):
        r.kx[:, i * ROWS : i * ROWS + ROWS] = r.kt[slot]
        r.vx[i * ROWS : i * ROWS + ROWS, :128] = r.va[slot]


def mix_all_rows(a, r):
    def one(xs, carry):
        for t in range(2 * ROWS // TILE):
            attend_rows(r, xs, slice(t * TILE, t * TILE + TILE))
        return carry

    lax.fori_loop(0, NX, one, 0)


def part_copies(a, r, d):
    x = around(a.x, d, NX)
    return (
        remote(r.ob.at[d], r.orc.at[d], r.o_ss.at[d], r.o_rs.at[d], x=x),
        remote(r.lb.at[d], r.lrc.at[d], r.l_ss.at[d], r.l_rs.at[d], x=x),
    )


def mix_last_rows(a, r):
    for d in X_ORDER:
        xs = around(a.x, d, NX)
        dst_o, dst_l = (r.ob, r.lb) if d else (r.orc, r.lrc)
        for t in range(2 * ROWS // TILE):
            at = slice(t * TILE, t * TILE + TILE)
            attend_rows(r, xs, at)
            acc = r.acc[xs, at, :]
            total = acc[:, 128:]
            dst_o[d, at, :] = (acc[:, :128] / total).astype(BF16)
            lse = r.mx[xs, at, :] + jnp.log2(total)
            for b in range(TILE // 128):
                row = t * (TILE // 128) + b
                dst_l[d, row : row + 1, :] = to_row(lse[b * 128 : b * 128 + 128, :])
        if d:
            for cp in part_copies(a, r, d):
                cp.start()


def mix_combine(a, r):
    for d in (1, 2, 3):
        for cp in part_copies(a, r, d):
            cp.wait_recv()
    for b in range(6):
        lse = [to_col(r.lrc[d, b : b + 1, :]) for d in range(NX)]
        top = functools.reduce(jnp.maximum, lse)
        w = [jnp.exp2(v - top) for v in lse]
        inv = 1.0 / functools.reduce(jnp.add, w)
        at = slice(b * 128, b * 128 + 128)
        o = None
        for d in range(NX):
            term = r.orc[d, at, :].astype(F32) * (w[d] * inv)
            o = term if o is None else o + term
        h, t = b // 3, b % 3
        r.att[t * 128 : t * 128 + 128, h * 128 : h * 128 + 128] = o.astype(BF16)


def project(r, half):
    for j in range(4):
        off = pl.multiple_of(half * 1024 + j * 256, 256)
        o = jnp.dot(r.att[...], r.wo[:, pl.ds(off, 256)], preferred_element_type=F32)
        r.mp[half, :, j * 256 : j * 256 + 256] = o.astype(BF16)


def mix_pair_copy(a, r):
    return remote(r.mp.at[1 - a.c], r.mr, r.m_ss.at[0], r.m_rs.at[0], c=1 - a.c)


def mix_sum_copy(a, r, d):
    y = around(a.y, d, NY)
    return remote(r.ms.at[y], r.yr.at[d], r.y_ss.at[d], r.y_rs.at[d], y=y)


def mix_project(a, r):
    pltpu.make_async_copy(r.wo_h, r.wo, r.wo_sem).wait()
    project(r, 1 - a.c)
    mix_pair_copy(a, r).start()
    project(r, a.c)
    mix_pair_copy(a, r).wait_recv()


def mix_scatter(a, r):
    for d in FAR_FIRST:
        y = around(a.y, d, NY)
        at = pl.ds(pl.multiple_of(y * 48, 16), 48)
        total = r.mp[a.c, at, :].astype(F32) + r.mr[at, :].astype(F32)
        if d:
            r.ms[y] = total.astype(BF16)
            mix_sum_copy(a, r, d).start()
        else:
            r.fs[...] = total


def mix_final_copy(a, r):
    src = r.fs.at[pl.ds(pl.multiple_of((1 - a.c) * 24, 8), 24)]
    return remote(src, r.fr, r.f_ss, r.f_rs, c=1 - a.c)


def mix_sum(a, r):
    total = r.fs[...]
    for d in range(1, NY):
        mix_sum_copy(a, r, d).wait_recv()
        total = total + r.yr[d].astype(F32)
    r.fs[...] = total
    mix_final_copy(a, r).start()


def mix_finish(a, r, out):
    mix_final_copy(a, r).wait()
    mine = r.fs[pl.ds(pl.multiple_of(a.c * 24, 8), 24), :]
    other = r.fr[...]
    sq = jnp.sum(mine * mine, axis=1, keepdims=True) + jnp.sum(other * other, axis=1, keepdims=True)
    inv = lax.rsqrt(sq * (1.0 / D) + EPS)
    for half, v in ((a.c, mine), (1 - a.c, other)):
        off = pl.ds(pl.multiple_of(half * 1024, 1024), 1024)
        out[:, off] = (v * inv * r.mgain[:, off]).astype(BF16)
    for d in (1, 2, 3):
        q_copy(a, r, d).wait_send()
        for cp in part_copies(a, r, d):
            cp.wait_send()
    for slot in range(OWN):
        for cp in kv_copies(a, r, slot):
            cp.wait_send()
    mix_pair_copy(a, r).wait_send()
    for d in range(1, NY):
        mix_sum_copy(a, r, d).wait_send()


def bind(names, refs):
    return SimpleNamespace(**dict(zip(names, refs, strict=True)))


def moe_kernel(*refs):
    r = bind((*MOE_IN, "out", *MOE_SCRATCH), refs)
    a = here()
    barrier = pltpu.get_barrier_semaphore()
    greet_ep(a, barrier)
    greet_tp(a, barrier, 2)
    moe_weights(r)
    moe_dispatch_build(a, r)
    pl.semaphore_wait(barrier, 46)
    exchange_start(a, r.disp, r.drecv, r.d_ss, r.d_rs)
    exchange_wait(r.disp, r.drecv, r.d_ss, r.d_rs)
    moe_compact(a, r)
    moe_gather_start(a, r)
    for i in (1, 2, 3):
        moe_gather_forward(a, r, i)
    moe_gather_finish(a, r)
    moe_experts(a, r)
    moe_pair_start(a, r)
    for i in range(NY):
        moe_pair_sum(a, r, i)
    moe_return_start(a, r)
    moe_combine(a, r)
    moe_finish(a, r, r.out)


def mix_kernel(*refs):
    r = bind((*MIX_IN, "out", *MIX_SCRATCH), refs)
    a = here()
    barrier = pltpu.get_barrier_semaphore()
    for d in (1, 2, 3):
        pl.semaphore_signal(barrier, inc=1, device_id={"x": around(a.x, d, NX)}, device_id_type=MESH_ID)
    for d in (1, -1):
        pl.semaphore_signal(barrier, inc=1, device_id={"z": around(a.z, d, NZ)}, device_id_type=MESH_ID)
    for d in range(1, NY):
        pl.semaphore_signal(barrier, inc=1, device_id={"y": around(a.y, d, NY)}, device_id_type=MESH_ID)
    pl.semaphore_signal(barrier, inc=1, device_id={"c": 1 - a.c}, device_id_type=MESH_ID)
    mix_turn(a, r)
    pl.semaphore_wait(barrier, 13)
    mix_send(a, r)
    for s in range(4):
        mix_step(a, r, s)
        if s == 0:
            for d in (1, 2, 3):
                q_copy(a, r, d).wait_recv()
        if s < 3:
            mix_all_rows(a, r)
    mix_last_rows(a, r)
    mix_combine(a, r)
    mix_project(a, r)
    mix_scatter(a, r)
    mix_sum(a, r)
    mix_finish(a, r, r.out)


def call(kernel, ins, hbm, scratch, out_shape, collective_id, flops):
    n = len(ins) - hbm
    return pl.pallas_call(
        kernel,
        out_shape=out_shape,
        in_specs=[pl.BlockSpec(memory_space=pltpu.VMEM)] * n + [pl.BlockSpec(memory_space=pl.ANY)] * hbm,
        out_specs=pl.BlockSpec(memory_space=pltpu.VMEM),
        scratch_shapes=list(scratch.values()),
        compiler_params=pltpu.CompilerParams(
            collective_id=collective_id, has_side_effects=True, vmem_limit_bytes=60 * 2**20
        ),
        cost_estimate=pl.CostEstimate(flops=flops, bytes_accessed=2**23, transcendentals=0),
    )(*ins)


def turn_tables():
    freq = (THETA ** (-np.arange(0, 64, 2, dtype=np.float32) / np.float32(64))).astype(np.float32)
    row = np.arange(192, dtype=np.float32)[:, None] * freq[None]
    col = np.arange(64, dtype=np.float32)[:, None] * freq[None]
    rowcs = np.zeros((2, 192, 128), np.float32)
    colcs = np.zeros((2, 64, 128), np.float32)
    rowcs[0, :, 0:32] = rowcs[0, :, 32:64] = np.cos(row)
    rowcs[1, :, 0:32], rowcs[1, :, 32:64] = -np.sin(row), np.sin(row)
    colcs[0, :, 64:96] = colcs[0, :, 96:128] = np.cos(col)
    colcs[1, :, 64:96], colcs[1, :, 96:128] = -np.sin(col), np.sin(col)
    return jnp.asarray(rowcs), jnp.asarray(colcs)


def slots_of(ids):
    flat = ids.reshape(-1)
    n = flat.shape[0]
    same = (flat[:, None] == flat[None, :]) & (iota((n, n), 1) < iota((n, n), 0))
    rank = jnp.sum(same.astype(jnp.int32), axis=1)
    return (flat * SLAB + rank).reshape(ids.shape)


def per_device(
    query_rows,
    key_rows,
    value_rows,
    query_gain,
    key_gain,
    w_out,
    mixer_gain,
    expert_input,
    expert_ids,
    expert_weights,
    input_gain,
    w_gate,
    w_up,
    w_down,
    out_gain,
):
    slots = slots_of(expert_ids)
    rowcs, colcs = turn_tables()
    scale = np.float32(np.log2(np.e) * HEAD**-0.5)
    moe_ins = (
        expert_input,
        slots.T,
        slots,
        expert_weights,
        input_gain.reshape(1, D),
        out_gain.reshape(1, 128),
        w_gate[0],
        w_up[0],
        w_down[0],
    )
    moe = call(
        moe_kernel, moe_ins, 3, MOE_SCRATCH, jax.ShapeDtypeStruct((TOKENS2, 128), BF16), 0, 2 * 10**9
    )
    mix_ins = (
        query_rows,
        key_rows,
        value_rows,
        (query_gain * scale).reshape(1, HEAD),
        key_gain.reshape(1, HEAD),
        rowcs,
        colcs,
        mixer_gain.reshape(1, D),
        w_out,
    )
    mix = call(mix_kernel, mix_ins, 1, MIX_SCRATCH, jax.ShapeDtypeStruct((24, D), BF16), 1, 10**10)
    return (mix, moe)


def solution(mesh):
    finer = Mesh(mesh.devices.reshape(NZ, NX, NY, NC), ("z", "x", "y", "c"))
    in_specs = (
        P(EP, TP),
        P(EP, TP),
        P(EP, TP),
        P(),
        P(),
        P(TP, None),
        P(),
        P(EP, None),
        P(EP, None),
        P(EP, None),
        P(),
        P(EP, None, TP),
        P(EP, None, TP),
        P(EP, TP, None),
        P(TP),
    )
    out_specs = (P(EP + TP, None), P(EP, TP))
    return jax.shard_map(
        per_device, mesh=finer, in_specs=in_specs, out_specs=out_specs, check_vma=False
    )
```

```python
import functools
from types import SimpleNamespace

import numpy as np
import jax
import jax.numpy as jnp
from jax import lax
from jax.experimental import pallas as pl
from jax.experimental.pallas import tpu as pltpu
from jax.sharding import Mesh
from jax.sharding import PartitionSpec as P

NZ, NX, NY, NC = 8, 4, 8, 2
EP = ("z", "x")
TP = ("y", "c")
D = 2048
HEAD = 128
GRID = 64
ROWS = 384
TOKENS2 = 192
CAP = 18
SLAB = 32
EXPERTS = 32
SLOTS = EXPERTS * CAP
PADDED = EXPERTS * SLAB
EPS = 1e-06
SCALE = float(np.log2(np.e) * HEAD**-0.5)
THETA = 10000.0
F32 = jnp.float32
BF16 = jnp.bfloat16
MESH_ID = pl.DeviceIdType.MESH
PAIR_ORDER = (3, -3, 4, 1, -1, 2, -2, 0)
ROLE_TO = (1, -1, 0, 1, -1, 2, -2)
SENT = 24
X_ORDER = (2, 1, 3, 0)


def around(i, d, n):
    return lax.rem(i + (d % n), n)


def here():
    a = SimpleNamespace()
    a.z, a.x, a.y, a.c = (lax.axis_index(n) for n in ("z", "x", "y", "c"))
    a.ep = a.z * NX + a.x
    return a


def remote(src, dst, ss, rs, **dev):
    return pltpu.make_async_remote_copy(
        src_ref=src, dst_ref=dst, send_sem=ss, recv_sem=rs, device_id=dev, device_id_type=MESH_ID
    )


def ep_peer(a, k):
    e = lax.rem(a.ep + k, EXPERTS)
    return e, lax.div(e, NX), lax.rem(e, NX)


def greet_ep(a, barrier):
    def one(k, carry):
        _, z, x = ep_peer(a, k)
        pl.semaphore_signal(barrier, inc=1, device_id={"z": z, "x": x}, device_id_type=MESH_ID)
        return carry

    lax.fori_loop(1, EXPERTS, one, 0)


def greet_tp(a, barrier):
    for d in range(NY):
        for o in range(2):
            if d or o:
                c = a.c if o == 0 else 1 - a.c
                pl.semaphore_signal(
                    barrier, inc=1, device_id={"y": around(a.y, d, NY), "c": c}, device_id_type=MESH_ID
                )


def wait_bytes(ref, sem):
    pltpu.make_async_copy(ref, ref, sem).wait()


def iota(shape, dim):
    return lax.broadcasted_iota(jnp.int32, shape, dim)


def eye128():
    return iota((128, 128), 0) == iota((128, 128), 1)


def to_row(col):
    return jnp.sum(jnp.where(eye128(), col, 0.0), axis=0, keepdims=True)


def to_col(row):
    return jnp.sum(jnp.where(eye128(), row, 0.0), axis=1, keepdims=True)


def tree_copy(a, src, relay, final, ss, rs, role):
    to = around(a.y, ROLE_TO[role], NY) if role != 2 else lax.rem(a.y + 2 + 4 * a.c, NY)
    dst = relay.at[role] if role < 3 else final.at[role - 3]
    return remote(src.at[around(a.y, PAIR_ORDER[role], NY)], dst, ss.at[role], rs.at[role], y=to)


def relayed(a, relay, role):
    share = jnp.where(a.c == 0, 1.0, 0.0) if role == 5 else jnp.where(a.c == 0, 0.0, 1.0)
    return relay[role - 5].astype(F32) + relay[2].astype(F32) * share


MOE_IN = ("xin", "ids", "wts", "igain", "ogain", "wg_h", "wu_h", "wd_h")
MOE_SCRATCH = dict(
    disp=pltpu.VMEM((EXPERTS, SLAB, 256), BF16),
    drecv=pltpu.VMEM((EXPERTS, SLAB, 256), BF16),
    xg=pltpu.VMEM((2, 4, 2, SLOTS, 128), BF16),
    xcat=pltpu.VMEM((SLOTS, D), BF16),
    wg=pltpu.VMEM((D, 256), BF16),
    wu=pltpu.VMEM((D, 256), BF16),
    wd=pltpu.VMEM((256, D), BF16),
    part=pltpu.VMEM((2, NY, SLOTS, 128), BF16),
    pr=pltpu.VMEM((NY, SLOTS, 128), BF16),
    ps=pltpu.VMEM((NY, SLOTS, 128), BF16),
    own=pltpu.VMEM((SLOTS, 128), F32),
    rs=pltpu.VMEM((4, SLOTS, 128), BF16),
    rl=pltpu.VMEM((3, SLOTS, 128), BF16),
    rsend=pltpu.VMEM((EXPERTS, SLAB, 128), BF16),
    rrecv=pltpu.VMEM((EXPERTS, SLAB, 128), BF16),
    comb=pltpu.VMEM((TOKENS2, 128), F32),
    scol=pltpu.VMEM((TOKENS2, 2), jnp.int32),
    sqs=pltpu.VMEM((8, 128), F32),
    sqr=pltpu.VMEM((16, 8, 128), F32),
    w_sem=pltpu.SemaphoreType.DMA((3,)),
    d_ss=pltpu.SemaphoreType.DMA,
    d_rs=pltpu.SemaphoreType.DMA,
    ag_ss=pltpu.SemaphoreType.DMA((3,)),
    ag_rs=pltpu.SemaphoreType.DMA((3,)),
    pf_ss=pltpu.SemaphoreType.DMA((4,)),
    pf_rs=pltpu.SemaphoreType.DMA((4,)),
    pp_ss=pltpu.SemaphoreType.DMA((8,)),
    pp_rs=pltpu.SemaphoreType.DMA((8,)),
    rs_ss=pltpu.SemaphoreType.DMA((8,)),
    rs_rs=pltpu.SemaphoreType.DMA((8,)),
    t_ss=pltpu.SemaphoreType.DMA,
    t_rs=pltpu.SemaphoreType.DMA,
    q_ss=pltpu.SemaphoreType.DMA,
    q_rs=pltpu.SemaphoreType.DMA,
)


def moe_weights(r):
    for i, (src, dst) in enumerate(((r.wg_h, r.wg), (r.wu_h, r.wu), (r.wd_h, r.wd))):
        pltpu.make_async_copy(src, dst, r.w_sem.at[i]).start()


def moe_weights_wait(r):
    for i, (src, dst) in enumerate(((r.wg_h, r.wg), (r.wu_h, r.wu), (r.wd_h, r.wd))):
        pltpu.make_async_copy(src, dst, r.w_sem.at[i]).wait()


def to_cols(row):
    return jnp.concatenate([to_col(row[:, :128]), to_col(row[:, 64:])[64:]], axis=0)


def moe_slots(r):
    rows = [r.ids[k : k + 1, :].astype(F32) for k in range(2)]
    cols = [to_cols(v) for v in rows]
    shape = (TOKENS2, TOKENS2)
    above, left = iota(shape, 0) < iota(shape, 1), iota(shape, 1) < iota(shape, 0)

    def rank(here, there, mask, dim):
        hits = [jnp.where((here == v) & mask, 1.0, 0.0) for v in there]
        return here * SLAB + jnp.sum(hits[0] + hits[1], axis=dim, keepdims=True)

    srow = [rank(v, cols, above, 0).astype(jnp.int32) for v in rows]
    scol = [rank(v, rows, left, 1).astype(jnp.int32) for v in cols]
    return srow, scol


def moe_dispatch_build(a, r):
    srow, scol = moe_slots(r)
    r.scol[...] = jnp.concatenate(scol, axis=1)
    x = r.xin[...].astype(F32)
    inv = lax.rsqrt(jnp.sum(x * x, axis=1, keepdims=True) * (1.0 / D) + EPS)
    g = lax.rem(a.y, 4)
    halves = []
    for j in range(2):
        off = pl.multiple_of(((g + 4 * j) * 2 + a.c) * 128, 128)
        xs = r.xin[:, pl.ds(off, 128)].astype(F32)
        halves.append((xs * inv * r.igain[:, pl.ds(off, 128)]).astype(BF16))
    nn = jnp.concatenate(halves, axis=1)
    rows = iota((PADDED, TOKENS2), 0)
    pick = (rows == srow[0]) | (rows == srow[1])
    pick = jnp.where(pick, 1.0, 0.0).astype(BF16)
    out = jnp.dot(pick, nn, preferred_element_type=F32).astype(BF16)
    r.disp[...] = out.reshape(EXPERTS, SLAB, 256)


def head(ref, e):
    return ref.at[e, pl.ds(0, SENT)]


def exchange_start(a, src, dst, ss, rs):
    def one(k, carry):
        e, z, x = ep_peer(a, k)
        remote(head(src, e), head(dst, a.ep), ss, rs, z=z, x=x).start()
        return carry

    lax.fori_loop(1, EXPERTS, one, 0)
    dst[a.ep] = src[a.ep]


def exchange_wait(src, dst, ss, rs):
    wait_bytes(dst.at[pl.ds(0, EXPERTS - 1), pl.ds(0, SENT)], rs)
    wait_bytes(src.at[pl.ds(0, EXPERTS - 1), pl.ds(0, SENT)], ss)


def padded_place(i):
    e = ((i.astype(F32) + 0.5) * (1.0 / CAP)).astype(jnp.int32)
    return i + e * (SLAB - CAP)


def moe_compact(a, r):
    g = lax.rem(a.y, 4)
    place = padded_place(iota((SLOTS, 1), 0))
    pick = jnp.where(iota((SLOTS, PADDED), 1) == place, 1.0, 0.0).astype(BF16)
    got = r.drecv[...].reshape(PADDED, 256)
    out = jnp.dot(pick, got, preferred_element_type=F32).astype(BF16)
    r.xg[a.c, g, 0] = out[:, :128]
    r.xg[a.c, g, 1] = out[:, 128:]


def moe_gather_copy(a, r, i):
    src = r.xg.at[a.c, lax.rem(a.y, 4)]
    to = around(a.y, (1, -1)[i], NY) if i < 2 else lax.rem(a.y + 2 + 4 * a.c, NY)
    return remote(src, src, r.ag_ss.at[i], r.ag_rs.at[i], y=to)


def moe_group(a, i):
    g = lax.rem(a.y, 4)
    return g if i == 0 else around(g, (3, 1, 2)[i - 1], 4)


def moe_partner_copy(a, r, i):
    src = r.xg.at[a.c, moe_group(a, i)]
    return remote(src, src, r.pf_ss.at[i], r.pf_rs.at[i], c=1 - a.c)


def moe_gather_start(a, r):
    for i in range(3):
        moe_gather_copy(a, r, i).start()
    moe_partner_copy(a, r, 0).start()


def moe_gather_forward(a, r, i):
    moe_gather_copy(a, r, i - 1).wait_recv()
    moe_partner_copy(a, r, i).start()


def moe_gather_finish(a, r):
    for i in range(3):
        moe_gather_copy(a, r, i).wait_send()
    for i in range(4):
        moe_partner_copy(a, r, i).wait()


def moe_experts(a, r):
    for par in range(2):
        for g in range(4):
            for h in range(2):
                at = ((g + 4 * h) * 2 + par) * 128
                r.xcat[:, at : at + 128] = r.xg[par, g, h]
    moe_weights_wait(r)

    def block(b, carry):
        at = pl.ds(pl.multiple_of(b * 192, 192), 192)
        xb = r.xcat[at, :]
        gate = jnp.dot(xb, r.wg[...], preferred_element_type=F32)
        up = jnp.dot(xb, r.wu[...], preferred_element_type=F32)
        hid = (gate / (1.0 + jnp.exp(-gate)) * up).astype(BF16)
        for ys in range(NY):
            o = jnp.dot(hid, r.wd[:, ys * 256 : ys * 256 + 256], preferred_element_type=F32)
            o = o.astype(BF16)
            r.part[0, ys, at, :] = o[:, :128]
            r.part[1, ys, at, :] = o[:, 128:]
        return carry

    lax.fori_loop(0, SLOTS // 192, block, 0)


def moe_pair_copy(a, r, i):
    ys = around(a.y, PAIR_ORDER[i], NY)
    return remote(r.part.at[1 - a.c, ys], r.pr.at[ys], r.pp_ss.at[i], r.pp_rs.at[i], c=1 - a.c)


def moe_tree_copy(a, r, role):
    return tree_copy(a, r.ps, r.rl, r.rs, r.rs_ss, r.rs_rs, role)


def moe_pair_start(a, r):
    for i in range(NY):
        moe_pair_copy(a, r, i).start()


def moe_pair_total(a, r, i):
    ys = around(a.y, PAIR_ORDER[i], NY)
    moe_pair_copy(a, r, i).wait_recv()
    return ys, r.part[a.c, ys].astype(F32) + r.pr[ys].astype(F32)


def moe_pair_sums(a, r):
    for role in range(5):
        ys, total = moe_pair_total(a, r, role)
        r.ps[ys] = total.astype(BF16)
        moe_tree_copy(a, r, role).start()
    r.own[...] = moe_pair_total(a, r, 7)[1]


def moe_relay(a, r):
    moe_tree_copy(a, r, 2).wait_recv()
    for role in (5, 6):
        ys, total = moe_pair_total(a, r, role)
        moe_tree_copy(a, r, role - 5).wait_recv()
        r.ps[ys] = (total + relayed(a, r.rl, role)).astype(BF16)
        moe_tree_copy(a, r, role).start()


def moe_return_start(a, r):
    total = r.own[...]
    for role in range(3, 7):
        moe_tree_copy(a, r, role).wait_recv()
        total = total + r.rs[role - 3].astype(F32)
    rows = total.astype(BF16)
    place = padded_place(iota((1, SLOTS), 1))
    pick = jnp.where(iota((PADDED, SLOTS), 0) == place, 1.0, 0.0).astype(BF16)
    out = jnp.dot(pick, rows, preferred_element_type=F32).astype(BF16)
    r.rsend[...] = out.reshape(EXPERTS, SLAB, 128)
    exchange_start(a, r.rsend, r.rrecv, r.t_ss, r.t_rs)


def square_targets(a):
    out = []
    for d in range(NY):
        for o in range(2):
            if d or o:
                out.append((around(a.y, d, NY), a.c if o == 0 else 1 - a.c))
    return out


def moe_combine(a, r):
    exchange_wait(r.rsend, r.rrecv, r.t_ss, r.t_rs)
    got = r.rrecv[...].reshape(PADDED, 128)
    total = None
    for k in range(2):
        pick = jnp.where(iota((TOKENS2, PADDED), 1) == r.scol[:, k : k + 1], 1.0, 0.0).astype(BF16)
        term = jnp.dot(pick, got, preferred_element_type=F32) * to_cols(r.wts[k : k + 1, :])
        total = term if total is None else total + term
    r.comb[...] = total
    sq = jnp.sum(total * total, axis=1, keepdims=True)
    r.sqs[...] = jnp.zeros((8, 128), F32)
    r.sqs[0:1, :] = to_row(sq[:128])
    r.sqs[1:2, :] = to_row(sq[64:])
    tp = a.y * 2 + a.c
    for y, c in square_targets(a):
        remote(r.sqs, r.sqr.at[tp], r.q_ss, r.q_rs, y=y, c=c).start()
    r.sqr[tp] = r.sqs[...]


def moe_finish(a, r, out):
    wait_bytes(r.sqr.at[pl.ds(0, 15)], r.q_rs)
    wait_bytes(r.sqr.at[pl.ds(0, 15)], r.q_ss)
    tot = r.sqr[0]
    for i in range(1, 16):
        tot = tot + r.sqr[i]
    inv = lax.rsqrt(tot * (1.0 / D) + EPS)
    lo, hi = to_col(inv[0:1, :]), to_col(inv[1:2, :])
    out[0:128, :] = (r.comb[0:128, :] * lo * r.ogain[...]).astype(BF16)
    out[128:192, :] = (r.comb[128:192, :] * hi[64:] * r.ogain[...]).astype(BF16)
    for role in range(7):
        moe_tree_copy(a, r, role).wait_send()
    for i in range(NY):
        moe_pair_copy(a, r, i).wait_send()


MIX_IN = ("q_in", "k_in", "v_in", "qg", "kg", "rowcs", "colcs", "mgain", "wo_h")
MIX_SCRATCH = dict(
    q_all=pltpu.VMEM((NX, 2 * ROWS, HEAD), BF16),
    kt=pltpu.VMEM((NZ, HEAD, ROWS), BF16),
    va=pltpu.VMEM((NZ, ROWS, HEAD), BF16),
    kx=pltpu.VMEM((HEAD, 2 * ROWS), BF16),
    vx=pltpu.VMEM((2 * ROWS, 256), BF16),
    mx=pltpu.VMEM((NX, 2 * ROWS, 128), F32),
    acc=pltpu.VMEM((NX, 2 * ROWS, 256), F32),
    ob=pltpu.VMEM((NX, 2 * ROWS, HEAD), BF16),
    lb=pltpu.VMEM((NX, 8, 128), F32),
    orc=pltpu.VMEM((NX, 2 * ROWS, HEAD), BF16),
    lrc=pltpu.VMEM((NX, 8, 128), F32),
    att=pltpu.VMEM((ROWS, 256), BF16),
    wo=pltpu.VMEM((256, D), BF16),
    mp=pltpu.VMEM((2, ROWS, 1024), BF16),
    mr=pltpu.VMEM((ROWS, 1024), BF16),
    ms=pltpu.VMEM((NY, 48, 1024), BF16),
    yr=pltpu.VMEM((4, 48, 1024), BF16),
    yl=pltpu.VMEM((3, 48, 1024), BF16),
    fs=pltpu.VMEM((48, 1024), F32),
    fr=pltpu.VMEM((24, 1024), F32),
    wo_sem=pltpu.SemaphoreType.DMA,
    xq_ss=pltpu.SemaphoreType.DMA((4,)),
    xq_rs=pltpu.SemaphoreType.DMA((4,)),
    k_ss=pltpu.SemaphoreType.DMA((8,)),
    k_rs=pltpu.SemaphoreType.DMA((8,)),
    v_ss=pltpu.SemaphoreType.DMA((8,)),
    v_rs=pltpu.SemaphoreType.DMA((8,)),
    o_ss=pltpu.SemaphoreType.DMA((4,)),
    o_rs=pltpu.SemaphoreType.DMA((4,)),
    l_ss=pltpu.SemaphoreType.DMA((4,)),
    l_rs=pltpu.SemaphoreType.DMA((4,)),
    m_ss=pltpu.SemaphoreType.DMA((2,)),
    m_rs=pltpu.SemaphoreType.DMA((2,)),
    y_ss=pltpu.SemaphoreType.DMA((8,)),
    y_rs=pltpu.SemaphoreType.DMA((8,)),
    f_ss=pltpu.SemaphoreType.DMA,
    f_rs=pltpu.SemaphoreType.DMA,
)
OWN = 7


def swap_parts(v):
    lane = lax.rem(iota(v.shape, 1), 64)
    return jnp.where(lane < 32, pltpu.roll(v, 96, 1), pltpu.roll(v, 32, 1))


def turned(a, r, block, gain, g):
    v = block.astype(F32)
    v = v * lax.rsqrt(jnp.mean(v * v, axis=1, keepdims=True) + EPS) * gain
    at = a.ep * (ROWS // GRID) + g
    cos = r.rowcs[0, pl.ds(at, 1), :] + r.colcs[0]
    sin = r.rowcs[1, pl.ds(at, 1), :] + r.colcs[1]
    return (v * cos + swap_parts(v) * sin).astype(BF16)


def mix_turn(a, r):
    pltpu.make_async_copy(r.wo_h, r.wo, r.wo_sem).start()
    keys = []
    for g in range(ROWS // GRID):
        at = slice(g * GRID, g * GRID + GRID)
        for h in range(2):
            q = turned(a, r, r.q_in[at, h * 128 : h * 128 + 128], r.qg[...] * SCALE, g)
            r.q_all[a.x, h * ROWS + g * GRID : h * ROWS + g * GRID + GRID, :] = q
        keys.append(turned(a, r, r.k_in[at, :], r.kg[...], g))
    key = jnp.concatenate(keys, axis=0)
    r.kt[OWN] = key.astype(F32).T.astype(BF16)
    r.va[OWN] = r.v_in[...]
    r.vx[:, 128:] = jnp.ones((2 * ROWS, 128), BF16)
    r.mx[...] = jnp.full(r.mx.shape, -1e30, F32)
    r.acc[...] = jnp.zeros(r.acc.shape, F32)


def q_copy(a, r, d):
    mine = r.q_all.at[a.x]
    return remote(mine, mine, r.xq_ss.at[d], r.xq_rs.at[d], x=around(a.x, d, NX))


def kv_copies(a, r, slot):
    src = OWN if slot < 2 else slot - 2
    z = around(a.z, 1 if slot % 2 == 0 else -1, NZ)
    return (
        remote(r.kt.at[src], r.kt.at[slot], r.k_ss.at[slot], r.k_rs.at[slot], z=z),
        remote(r.va.at[src], r.va.at[slot], r.v_ss.at[slot], r.v_rs.at[slot], z=z),
    )


def kv_start(a, r, slot):
    for cp in kv_copies(a, r, slot):
        cp.start()


def kv_arrived(a, r, slot):
    for cp in kv_copies(a, r, slot):
        cp.wait_recv()
    if slot + 2 < OWN:
        kv_start(a, r, slot + 2)


def mix_send(a, r):
    kv_start(a, r, 0)
    kv_start(a, r, 1)
    for d in (2, 1, 3):
        q_copy(a, r, d).start()


def attend_rows(r, xs, at):
    q = r.q_all[xs, at, :]
    s = jnp.dot(q, r.kx[...], preferred_element_type=F32)
    old = r.mx[xs, at, :]
    new = jnp.maximum(old, jnp.max(s, axis=1, keepdims=True))
    r.mx[xs, at, :] = new
    p = jnp.concatenate(
        [jnp.exp2(s[:, j * 128 : j * 128 + 128] - new).astype(BF16) for j in range(6)], axis=1
    )
    keep = jnp.exp2(old - new)
    pv = jnp.dot(p, r.vx[...], preferred_element_type=F32)
    acc = r.acc[xs, at, :]
    r.acc[xs, at, :] = acc * jnp.concatenate([keep, keep], axis=1) + pv


TILE = 256


def mix_step(a, r, s):
    slots = (2 * s, 2 * s + 1)
    for slot in slots:
        if slot != OWN:
            kv_arrived(a, r, slot)
    for i, slot in enumerate(slots):
        r.kx[:, i * ROWS : i * ROWS + ROWS] = r.kt[slot]
        r.vx[i * ROWS : i * ROWS + ROWS, :128] = r.va[slot]


def mix_all_rows(a, r):
    def one(xs, carry):
        for t in range(2 * ROWS // TILE):
            attend_rows(r, xs, slice(t * TILE, t * TILE + TILE))
        return carry

    lax.fori_loop(0, NX, one, 0)


def part_copies(a, r, d):
    x = around(a.x, d, NX)
    return (
        remote(r.ob.at[d], r.orc.at[d], r.o_ss.at[d], r.o_rs.at[d], x=x),
        remote(r.lb.at[d], r.lrc.at[d], r.l_ss.at[d], r.l_rs.at[d], x=x),
    )


def mix_last_rows(a, r, d):
    xs = around(a.x, d, NX)
    dst_o, dst_l = (r.ob, r.lb) if d else (r.orc, r.lrc)
    for t in range(2 * ROWS // TILE):
        at = slice(t * TILE, t * TILE + TILE)
        attend_rows(r, xs, at)
        acc = r.acc[xs, at, :]
        total = acc[:, 128:]
        dst_o[d, at, :] = (acc[:, :128] / total).astype(BF16)
        lse = r.mx[xs, at, :] + jnp.log2(total)
        for b in range(TILE // 128):
            row = t * (TILE // 128) + b
            dst_l[d, row : row + 1, :] = to_row(lse[b * 128 : b * 128 + 128, :])
    if d:
        for cp in part_copies(a, r, d):
            cp.start()


def mix_combine(a, r):
    for d in (1, 2, 3):
        for cp in part_copies(a, r, d):
            cp.wait_recv()
    for b in range(6):
        lse = [to_col(r.lrc[d, b : b + 1, :]) for d in range(NX)]
        top = functools.reduce(jnp.maximum, lse)
        w = [jnp.exp2(v - top) for v in lse]
        inv = 1.0 / functools.reduce(jnp.add, w)
        at = slice(b * 128, b * 128 + 128)
        o = None
        for d in range(NX):
            term = r.orc[d, at, :].astype(F32) * (w[d] * inv)
            o = term if o is None else o + term
        h, t = b // 3, b % 3
        r.att[t * 128 : t * 128 + 128, h * 128 : h * 128 + 128] = o.astype(BF16)


def project(r, half):
    for j in range(4):
        off = pl.multiple_of(half * 1024 + j * 256, 256)
        o = jnp.dot(r.att[...], r.wo[:, pl.ds(off, 256)], preferred_element_type=F32)
        r.mp[half, :, j * 256 : j * 256 + 256] = o.astype(BF16)


def mix_pair_copy(a, r):
    return remote(r.mp.at[1 - a.c], r.mr, r.m_ss.at[0], r.m_rs.at[0], c=1 - a.c)


def mix_tree_copy(a, r, role):
    return tree_copy(a, r.ms, r.yl, r.yr, r.y_ss, r.y_rs, role)


def mix_project(a, r):
    pltpu.make_async_copy(r.wo_h, r.wo, r.wo_sem).wait()
    project(r, 1 - a.c)
    mix_pair_copy(a, r).start()
    project(r, a.c)
    mix_pair_copy(a, r).wait_recv()


def mix_pair_total(a, r, i):
    y = around(a.y, PAIR_ORDER[i], NY)
    at = pl.ds(pl.multiple_of(y * 48, 16), 48)
    return y, r.mp[a.c, at, :].astype(F32) + r.mr[at, :].astype(F32)


def mix_scatter(a, r):
    for role in range(5):
        y, total = mix_pair_total(a, r, role)
        r.ms[y] = total.astype(BF16)
        mix_tree_copy(a, r, role).start()
    r.fs[...] = mix_pair_total(a, r, 7)[1]


def mix_relay(a, r):
    mix_tree_copy(a, r, 2).wait_recv()
    for role in (5, 6):
        y, total = mix_pair_total(a, r, role)
        mix_tree_copy(a, r, role - 5).wait_recv()
        r.ms[y] = (total + relayed(a, r.yl, role)).astype(BF16)
        mix_tree_copy(a, r, role).start()


def mix_final_copy(a, r):
    src = r.fs.at[pl.ds(pl.multiple_of((1 - a.c) * 24, 8), 24)]
    return remote(src, r.fr, r.f_ss, r.f_rs, c=1 - a.c)


def mix_sum(a, r):
    total = r.fs[...]
    for role in range(3, 7):
        mix_tree_copy(a, r, role).wait_recv()
        total = total + r.yr[role - 3].astype(F32)
    r.fs[...] = total
    mix_final_copy(a, r).start()


def mix_finish(a, r, out):
    mix_final_copy(a, r).wait()
    mine = r.fs[pl.ds(pl.multiple_of(a.c * 24, 8), 24), :]
    other = r.fr[...]
    sq = jnp.sum(mine * mine, axis=1, keepdims=True) + jnp.sum(other * other, axis=1, keepdims=True)
    inv = lax.rsqrt(sq * (1.0 / D) + EPS)
    for half, v in ((a.c, mine), (1 - a.c, other)):
        off = pl.ds(pl.multiple_of(half * 1024, 1024), 1024)
        out[:, off] = (v * inv * r.mgain[:, off]).astype(BF16)
    for d in (1, 2, 3):
        q_copy(a, r, d).wait_send()
        for cp in part_copies(a, r, d):
            cp.wait_send()
    for slot in range(OWN):
        for cp in kv_copies(a, r, slot):
            cp.wait_send()
    mix_pair_copy(a, r).wait_send()
    for role in range(7):
        mix_tree_copy(a, r, role).wait_send()


def bind(names, refs):
    return SimpleNamespace(**dict(zip(names, refs, strict=True)))


def kernel(*refs):
    r = bind((*MOE_IN[:-3], *MIX_IN[:-1], *MOE_IN[-3:], MIX_IN[-1], "moe_out", "mix_out", *SCRATCH), refs)
    a = here()
    r.drecv[...] = jnp.zeros(r.drecv.shape, BF16)
    r.rrecv[...] = jnp.zeros(r.rrecv.shape, BF16)
    barrier = pltpu.get_barrier_semaphore()
    greet_ep(a, barrier)
    greet_tp(a, barrier)
    moe_weights(r)
    moe_dispatch_build(a, r)
    pl.semaphore_wait(barrier, 46)
    exchange_start(a, r.disp, r.drecv, r.d_ss, r.d_rs)
    mix_turn(a, r)
    mix_send(a, r)
    exchange_wait(r.disp, r.drecv, r.d_ss, r.d_rs)
    moe_compact(a, r)
    moe_gather_start(a, r)
    mix_step(a, r, 0)
    for d in (1, 2, 3):
        q_copy(a, r, d).wait_recv()
    mix_all_rows(a, r)
    mix_step(a, r, 1)
    mix_all_rows(a, r)
    moe_gather_forward(a, r, 1)
    moe_gather_forward(a, r, 2)
    moe_gather_forward(a, r, 3)
    mix_step(a, r, 2)
    moe_gather_finish(a, r)
    moe_experts(a, r)
    moe_pair_start(a, r)
    mix_all_rows(a, r)
    moe_pair_sums(a, r)
    mix_step(a, r, 3)
    mix_last_rows(a, r, 2)
    mix_last_rows(a, r, 1)
    moe_relay(a, r)
    mix_last_rows(a, r, 3)
    mix_last_rows(a, r, 0)
    mix_combine(a, r)
    mix_project(a, r)
    mix_scatter(a, r)
    moe_return_start(a, r)
    mix_relay(a, r)
    moe_combine(a, r)
    mix_sum(a, r)
    moe_finish(a, r, r.moe_out)
    mix_finish(a, r, r.mix_out)


SCRATCH = MOE_SCRATCH | MIX_SCRATCH


def call(ins, hbm):
    n = len(ins) - hbm
    return pl.pallas_call(
        kernel,
        out_shape=(jax.ShapeDtypeStruct((TOKENS2, 128), BF16), jax.ShapeDtypeStruct((24, D), BF16)),
        in_specs=[pl.BlockSpec(memory_space=pltpu.VMEM)] * n + [pl.BlockSpec(memory_space=pl.ANY)] * hbm,
        out_specs=(pl.BlockSpec(memory_space=pltpu.VMEM),) * 2,
        scratch_shapes=list(SCRATCH.values()),
        compiler_params=pltpu.CompilerParams(
            collective_id=0, has_side_effects=True, vmem_limit_bytes=60 * 2**20
        ),
        cost_estimate=pl.CostEstimate(flops=10**10, bytes_accessed=2**23, transcendentals=0),
    )(*ins)


def turn_tables():
    freq = (THETA ** (-np.arange(0, 64, 2, dtype=np.float32) / np.float32(64))).astype(np.float32)
    row = np.arange(192, dtype=np.float32)[:, None] * freq[None]
    col = np.arange(64, dtype=np.float32)[:, None] * freq[None]
    rowcs = np.zeros((2, 192, 128), np.float32)
    colcs = np.zeros((2, 64, 128), np.float32)
    rowcs[0, :, 0:32] = rowcs[0, :, 32:64] = np.cos(row)
    rowcs[1, :, 0:32], rowcs[1, :, 32:64] = -np.sin(row), np.sin(row)
    colcs[0, :, 64:96] = colcs[0, :, 96:128] = np.cos(col)
    colcs[1, :, 64:96], colcs[1, :, 96:128] = -np.sin(col), np.sin(col)
    return jnp.asarray(rowcs), jnp.asarray(colcs)


def per_device(
    query_rows,
    key_rows,
    value_rows,
    query_gain,
    key_gain,
    w_out,
    mixer_gain,
    expert_input,
    expert_ids,
    expert_weights,
    input_gain,
    w_gate,
    w_up,
    w_down,
    out_gain,
):
    rowcs, colcs = turn_tables()
    moe, mix = call(
        (
            expert_input,
            expert_ids.T,
            expert_weights.T,
            input_gain.reshape(1, D),
            out_gain.reshape(1, 128),
            query_rows,
            key_rows,
            value_rows,
            query_gain.reshape(1, HEAD),
            key_gain.reshape(1, HEAD),
            rowcs,
            colcs,
            mixer_gain.reshape(1, D),
            w_gate[0],
            w_up[0],
            w_down[0],
            w_out,
        ),
        4,
    )
    return (mix, moe)


def solution(mesh):
    finer = Mesh(mesh.devices.reshape(NZ, NX, NY, NC), ("z", "x", "y", "c"))
    in_specs = (
        P(EP, TP),
        P(EP, TP),
        P(EP, TP),
        P(),
        P(),
        P(TP, None),
        P(),
        P(EP, None),
        P(EP, None),
        P(EP, None),
        P(),
        P(EP, None, TP),
        P(EP, None, TP),
        P(EP, TP, None),
        P(TP),
    )
    out_specs = (P(EP + TP, None), P(EP, TP))
    return jax.shard_map(
        per_device, mesh=finer, in_specs=in_specs, out_specs=out_specs, check_vma=False
    )
```

```python
import functools
from types import SimpleNamespace

import numpy as np
import jax
import jax.numpy as jnp
from jax import lax
from jax.experimental import pallas as pl
from jax.experimental.pallas import tpu as pltpu
from jax.sharding import Mesh
from jax.sharding import PartitionSpec as P

NZ, NX, NY, NC = 8, 4, 8, 2
EP = ("z", "x")
TP = ("y", "c")
D = 2048
HEAD = 128
GRID = 64
ROWS = 384
TOKENS2 = 192
CAP = 18
SLAB = 32
EXPERTS = 32
SLOTS = EXPERTS * CAP
PADDED = EXPERTS * SLAB
EPS = 1e-06
SCALE = float(np.log2(np.e) * HEAD**-0.5)
THETA = 10000.0
F32 = jnp.float32
BF16 = jnp.bfloat16
MESH_ID = pl.DeviceIdType.MESH
PAIR_ORDER = (3, -3, 4, 1, -1, 2, -2, 0)
ROLE_TO = (1, -1, 0, 1, -1, 2, -2)
SENT = 24
BLOCKS = 3
BLOCK = 192
X_ORDER = (2, 1, 3, 0)


def around(i, d, n):
    return lax.rem(i + (d % n), n)


def here():
    a = SimpleNamespace()
    a.z, a.x, a.y, a.c = (lax.axis_index(n) for n in ("z", "x", "y", "c"))
    a.ep = a.z * NX + a.x
    return a


def remote(src, dst, ss, rs, **dev):
    return pltpu.make_async_remote_copy(
        src_ref=src, dst_ref=dst, send_sem=ss, recv_sem=rs, device_id=dev, device_id_type=MESH_ID
    )


def ep_peer(a, k):
    e = lax.rem(a.ep + k, EXPERTS)
    return e, lax.div(e, NX), lax.rem(e, NX)


def greet_ep(a, barrier):
    def one(k, carry):
        _, z, x = ep_peer(a, k)
        pl.semaphore_signal(barrier, inc=1, device_id={"z": z, "x": x}, device_id_type=MESH_ID)
        return carry

    lax.fori_loop(1, EXPERTS, one, 0)


def greet_tp(a, barrier):
    for d in range(NY):
        for o in range(2):
            if d or o:
                c = a.c if o == 0 else 1 - a.c
                pl.semaphore_signal(
                    barrier, inc=1, device_id={"y": around(a.y, d, NY), "c": c}, device_id_type=MESH_ID
                )


def wait_bytes(ref, sem):
    pltpu.make_async_copy(ref, ref, sem).wait()


def iota(shape, dim):
    return lax.broadcasted_iota(jnp.int32, shape, dim)


def eye128():
    return iota((128, 128), 0) == iota((128, 128), 1)


def to_row(col):
    return jnp.sum(jnp.where(eye128(), col, 0.0), axis=0, keepdims=True)


def to_col(row):
    return jnp.sum(jnp.where(eye128(), row, 0.0), axis=1, keepdims=True)


def tree_copy(a, src, relay, final, ss, rs, role, at=()):
    to = around(a.y, ROLE_TO[role], NY) if role != 2 else lax.rem(a.y + 2 + 4 * a.c, NY)
    dst = relay.at[(role, *at)] if role < 3 else final.at[(role - 3, *at)]
    mine = src.at[(around(a.y, PAIR_ORDER[role], NY), *at)]
    return remote(mine, dst, ss.at[(*at, role)], rs.at[(*at, role)], y=to)


def relayed(a, relay, role, at=()):
    share = jnp.where(a.c == 0, 1.0, 0.0) if role == 5 else jnp.where(a.c == 0, 0.0, 1.0)
    return relay[(role - 5, *at)].astype(F32) + relay[(2, *at)].astype(F32) * share


MOE_IN = ("xin", "ids", "wts", "igain", "ogain", "wg_h", "wu_h", "wd_h")
MOE_SCRATCH = dict(
    disp=pltpu.VMEM((EXPERTS, SLAB, 256), BF16),
    drecv=pltpu.VMEM((EXPERTS, SLAB, 256), BF16),
    xg=pltpu.VMEM((2, 4, BLOCKS, 2, BLOCK, 128), BF16),
    xcat=pltpu.VMEM((BLOCK, D), BF16),
    wg=pltpu.VMEM((D, 256), BF16),
    wu=pltpu.VMEM((D, 256), BF16),
    wd=pltpu.VMEM((256, D), BF16),
    part=pltpu.VMEM((2, NY, BLOCKS, BLOCK, 128), BF16),
    pr=pltpu.VMEM((NY, BLOCKS, BLOCK, 128), BF16),
    ps=pltpu.VMEM((NY, BLOCKS, BLOCK, 128), BF16),
    own=pltpu.VMEM((BLOCKS, BLOCK, 128), F32),
    rs=pltpu.VMEM((4, BLOCKS, BLOCK, 128), BF16),
    rl=pltpu.VMEM((3, BLOCKS, BLOCK, 128), BF16),
    rsend=pltpu.VMEM((EXPERTS, SLAB, 128), BF16),
    rrecv=pltpu.VMEM((EXPERTS, SLAB, 128), BF16),
    comb=pltpu.VMEM((TOKENS2, 128), F32),
    scol=pltpu.VMEM((TOKENS2, 2), jnp.int32),
    sqs=pltpu.VMEM((8, 128), F32),
    sqr=pltpu.VMEM((16, 8, 128), F32),
    w_sem=pltpu.SemaphoreType.DMA((3,)),
    d_ss=pltpu.SemaphoreType.DMA,
    d_rs=pltpu.SemaphoreType.DMA,
    ag_ss=pltpu.SemaphoreType.DMA((BLOCKS, 3)),
    ag_rs=pltpu.SemaphoreType.DMA((BLOCKS, 3)),
    pf_ss=pltpu.SemaphoreType.DMA((BLOCKS, 4)),
    pf_rs=pltpu.SemaphoreType.DMA((BLOCKS, 4)),
    pp_ss=pltpu.SemaphoreType.DMA((BLOCKS, 8)),
    pp_rs=pltpu.SemaphoreType.DMA((BLOCKS, 8)),
    rs_ss=pltpu.SemaphoreType.DMA((BLOCKS, 8)),
    rs_rs=pltpu.SemaphoreType.DMA((BLOCKS, 8)),
    t_ss=pltpu.SemaphoreType.DMA,
    t_rs=pltpu.SemaphoreType.DMA,
    q_ss=pltpu.SemaphoreType.DMA,
    q_rs=pltpu.SemaphoreType.DMA,
)


def moe_weights(r):
    for i, (src, dst) in enumerate(((r.wg_h, r.wg), (r.wu_h, r.wu), (r.wd_h, r.wd))):
        pltpu.make_async_copy(src, dst, r.w_sem.at[i]).start()


def moe_weights_wait(r):
    for i, (src, dst) in enumerate(((r.wg_h, r.wg), (r.wu_h, r.wu), (r.wd_h, r.wd))):
        pltpu.make_async_copy(src, dst, r.w_sem.at[i]).wait()


def to_cols(row):
    return jnp.concatenate([to_col(row[:, :128]), to_col(row[:, 64:])[64:]], axis=0)


def moe_slots(r):
    rows = [r.ids[k : k + 1, :].astype(F32) for k in range(2)]
    cols = [to_cols(v) for v in rows]
    shape = (TOKENS2, TOKENS2)
    above, left = iota(shape, 0) < iota(shape, 1), iota(shape, 1) < iota(shape, 0)

    def rank(here, there, mask, dim):
        hits = [jnp.where((here == v) & mask, 1.0, 0.0) for v in there]
        return here * SLAB + jnp.sum(hits[0] + hits[1], axis=dim, keepdims=True)

    srow = [rank(v, cols, above, 0).astype(jnp.int32) for v in rows]
    scol = [rank(v, rows, left, 1).astype(jnp.int32) for v in cols]
    return srow, scol


def moe_dispatch_build(a, r):
    srow, scol = moe_slots(r)
    r.scol[...] = jnp.concatenate(scol, axis=1)
    x = r.xin[...].astype(F32)
    inv = lax.rsqrt(jnp.sum(x * x, axis=1, keepdims=True) * (1.0 / D) + EPS)
    g = lax.rem(a.y, 4)
    halves = []
    for j in range(2):
        off = pl.multiple_of(((g + 4 * j) * 2 + a.c) * 128, 128)
        xs = r.xin[:, pl.ds(off, 128)].astype(F32)
        halves.append((xs * inv * r.igain[:, pl.ds(off, 128)]).astype(BF16))
    nn = jnp.concatenate(halves, axis=1)
    rows = iota((PADDED, TOKENS2), 0)
    pick = (rows == srow[0]) | (rows == srow[1])
    pick = jnp.where(pick, 1.0, 0.0).astype(BF16)
    out = jnp.dot(pick, nn, preferred_element_type=F32).astype(BF16)
    r.disp[...] = out.reshape(EXPERTS, SLAB, 256)


def head(ref, e):
    return ref.at[e, pl.ds(0, SENT)]


def exchange_start(a, src, dst, ss, rs):
    def one(k, carry):
        e, z, x = ep_peer(a, k)
        remote(head(src, e), head(dst, a.ep), ss, rs, z=z, x=x).start()
        return carry

    lax.fori_loop(1, EXPERTS, one, 0)
    dst[a.ep] = src[a.ep]


def exchange_wait(src, dst, ss, rs):
    wait_bytes(dst.at[pl.ds(0, EXPERTS - 1), pl.ds(0, SENT)], rs)
    wait_bytes(src.at[pl.ds(0, EXPERTS - 1), pl.ds(0, SENT)], ss)


def padded_place(i):
    e = ((i.astype(F32) + 0.5) * (1.0 / CAP)).astype(jnp.int32)
    return i + e * (SLAB - CAP)


def moe_compact(a, r):
    g = lax.rem(a.y, 4)
    place = padded_place(iota((SLOTS, 1), 0))
    pick = jnp.where(iota((SLOTS, PADDED), 1) == place, 1.0, 0.0).astype(BF16)
    got = r.drecv[...].reshape(PADDED, 256)
    out = jnp.dot(pick, got, preferred_element_type=F32).astype(BF16)
    for b in range(BLOCKS):
        for h in range(2):
            r.xg[a.c, g, b, h] = out[b * BLOCK : b * BLOCK + BLOCK, h * 128 : h * 128 + 128]


def moe_gather_copy(a, r, b, i):
    src = r.xg.at[a.c, lax.rem(a.y, 4), b]
    to = around(a.y, (1, -1)[i], NY) if i < 2 else lax.rem(a.y + 2 + 4 * a.c, NY)
    return remote(src, src, r.ag_ss.at[b, i], r.ag_rs.at[b, i], y=to)


def moe_group(a, i):
    return around(lax.rem(a.y, 4), (0, 3, 1, 2)[i], 4)


def moe_partner_copy(a, r, b, i):
    src = r.xg.at[a.c, moe_group(a, i), b]
    return remote(src, src, r.pf_ss.at[b, i], r.pf_rs.at[b, i], c=1 - a.c)


def moe_gather_start(a, r):
    for b in range(BLOCKS):
        for i in (2, 0, 1):
            moe_gather_copy(a, r, b, i).start()
    for b in range(BLOCKS):
        moe_partner_copy(a, r, b, 0).start()


def moe_gather_forward(a, r, b):
    for i in range(3):
        moe_gather_copy(a, r, b, i).wait_recv()
        moe_partner_copy(a, r, b, i + 1).start()


def moe_experts(a, r, b):
    for i in range(4):
        moe_partner_copy(a, r, b, i).wait_recv()
    for par in range(2):
        for g in range(4):
            for h in range(2):
                at = ((g + 4 * h) * 2 + par) * 128
                r.xcat[:, at : at + 128] = r.xg[par, g, b, h]
    if b == 0:
        moe_weights_wait(r)
    xb = r.xcat[...]
    gate = jnp.dot(xb, r.wg[...], preferred_element_type=F32)
    up = jnp.dot(xb, r.wu[...], preferred_element_type=F32)
    hid = (gate / (1.0 + jnp.exp(-gate)) * up).astype(BF16)
    for ys in range(NY):
        o = jnp.dot(hid, r.wd[:, ys * 256 : ys * 256 + 256], preferred_element_type=F32)
        o = o.astype(BF16)
        r.part[0, ys, b] = o[:, :128]
        r.part[1, ys, b] = o[:, 128:]
    for i in range(NY):
        moe_pair_copy(a, r, b, i).start()


def moe_pair_copy(a, r, b, i):
    ys = around(a.y, PAIR_ORDER[i], NY)
    return remote(r.part.at[1 - a.c, ys, b], r.pr.at[ys, b], r.pp_ss.at[b, i], r.pp_rs.at[b, i], c=1 - a.c)


def moe_tree_copy(a, r, b, role):
    return tree_copy(a, r.ps, r.rl, r.rs, r.rs_ss, r.rs_rs, role, (b,))


def moe_pair_total(a, r, b, i):
    ys = around(a.y, PAIR_ORDER[i], NY)
    moe_pair_copy(a, r, b, i).wait_recv()
    return ys, r.part[a.c, ys, b].astype(F32) + r.pr[ys, b].astype(F32)


def moe_pair_sums(a, r, b):
    for role in range(5):
        ys, total = moe_pair_total(a, r, b, role)
        r.ps[ys, b] = total.astype(BF16)
        moe_tree_copy(a, r, b, role).start()
    r.own[b] = moe_pair_total(a, r, b, 7)[1]


def moe_relay(a, r, b):
    moe_tree_copy(a, r, b, 2).wait_recv()
    for role in (5, 6):
        ys, total = moe_pair_total(a, r, b, role)
        moe_tree_copy(a, r, b, role - 5).wait_recv()
        r.ps[ys, b] = (total + relayed(a, r.rl, role, (b,))).astype(BF16)
        moe_tree_copy(a, r, b, role).start()


def moe_return_start(a, r):
    rows = []
    for b in range(BLOCKS):
        total = r.own[b]
        for role in range(3, 7):
            moe_tree_copy(a, r, b, role).wait_recv()
            total = total + r.rs[role - 3, b].astype(F32)
        rows.append(total.astype(BF16))
    rows = jnp.concatenate(rows, axis=0)
    place = padded_place(iota((1, SLOTS), 1))
    pick = jnp.where(iota((PADDED, SLOTS), 0) == place, 1.0, 0.0).astype(BF16)
    out = jnp.dot(pick, rows, preferred_element_type=F32).astype(BF16)
    r.rsend[...] = out.reshape(EXPERTS, SLAB, 128)
    exchange_start(a, r.rsend, r.rrecv, r.t_ss, r.t_rs)


def square_targets(a):
    out = []
    for d in range(NY):
        for o in range(2):
            if d or o:
                out.append((around(a.y, d, NY), a.c if o == 0 else 1 - a.c))
    return out


def moe_combine(a, r):
    exchange_wait(r.rsend, r.rrecv, r.t_ss, r.t_rs)
    got = r.rrecv[...].reshape(PADDED, 128)
    total = None
    for k in range(2):
        pick = jnp.where(iota((TOKENS2, PADDED), 1) == r.scol[:, k : k + 1], 1.0, 0.0).astype(BF16)
        term = jnp.dot(pick, got, preferred_element_type=F32) * to_cols(r.wts[k : k + 1, :])
        total = term if total is None else total + term
    r.comb[...] = total
    sq = jnp.sum(total * total, axis=1, keepdims=True)
    r.sqs[...] = jnp.zeros((8, 128), F32)
    r.sqs[0:1, :] = to_row(sq[:128])
    r.sqs[1:2, :] = to_row(sq[64:])
    tp = a.y * 2 + a.c
    for y, c in square_targets(a):
        remote(r.sqs, r.sqr.at[tp], r.q_ss, r.q_rs, y=y, c=c).start()
    r.sqr[tp] = r.sqs[...]


def moe_finish(a, r, out):
    wait_bytes(r.sqr.at[pl.ds(0, 15)], r.q_rs)
    wait_bytes(r.sqr.at[pl.ds(0, 15)], r.q_ss)
    tot = r.sqr[0]
    for i in range(1, 16):
        tot = tot + r.sqr[i]
    inv = lax.rsqrt(tot * (1.0 / D) + EPS)
    lo, hi = to_col(inv[0:1, :]), to_col(inv[1:2, :])
    out[0:128, :] = (r.comb[0:128, :] * lo * r.ogain[...]).astype(BF16)
    out[128:192, :] = (r.comb[128:192, :] * hi[64:] * r.ogain[...]).astype(BF16)
    for b in range(BLOCKS):
        for i in range(3):
            moe_gather_copy(a, r, b, i).wait_send()
        for i in range(4):
            moe_partner_copy(a, r, b, i).wait_send()
        for role in range(7):
            moe_tree_copy(a, r, b, role).wait_send()
        for i in range(NY):
            moe_pair_copy(a, r, b, i).wait_send()


MIX_IN = ("q_in", "k_in", "v_in", "qg", "kg", "rowcs", "colcs", "mgain", "wo_h")
MIX_SCRATCH = dict(
    q_all=pltpu.VMEM((NX, 2 * ROWS, HEAD), BF16),
    kt=pltpu.VMEM((NZ, HEAD, ROWS), BF16),
    va=pltpu.VMEM((NZ, ROWS, HEAD), BF16),
    kx=pltpu.VMEM((2, HEAD, 2 * ROWS), BF16),
    vx=pltpu.VMEM((2, 2 * ROWS, 256), BF16),
    mx=pltpu.VMEM((NX, 2 * ROWS, 128), F32),
    acc=pltpu.VMEM((NX, 2 * ROWS, 256), F32),
    ob=pltpu.VMEM((NX, 2, ROWS, HEAD), BF16),
    lb=pltpu.VMEM((NX, 2, 8, 128), F32),
    orc=pltpu.VMEM((NX, 2, ROWS, HEAD), BF16),
    lrc=pltpu.VMEM((NX, 2, 8, 128), F32),
    att=pltpu.VMEM((2, 2, ROWS, HEAD), BF16),
    wo=pltpu.VMEM((2, 256, 1024), BF16),
    mp=pltpu.VMEM((ROWS, 1024), F32),
    ms=pltpu.VMEM((NY, 48, 1024), BF16),
    yr=pltpu.VMEM((4, 48, 1024), BF16),
    yl=pltpu.VMEM((3, 48, 1024), BF16),
    fs=pltpu.VMEM((48, 1024), F32),
    fr=pltpu.VMEM((24, 1024), F32),
    wo_sem=pltpu.SemaphoreType.DMA,
    we_ss=pltpu.SemaphoreType.DMA,
    we_rs=pltpu.SemaphoreType.DMA,
    xq_ss=pltpu.SemaphoreType.DMA((4,)),
    xq_rs=pltpu.SemaphoreType.DMA((4,)),
    k_ss=pltpu.SemaphoreType.DMA((8,)),
    k_rs=pltpu.SemaphoreType.DMA((8,)),
    v_ss=pltpu.SemaphoreType.DMA((8,)),
    v_rs=pltpu.SemaphoreType.DMA((8,)),
    o_ss=pltpu.SemaphoreType.DMA((4, 2)),
    o_rs=pltpu.SemaphoreType.DMA((4, 2)),
    l_ss=pltpu.SemaphoreType.DMA((4, 2)),
    l_rs=pltpu.SemaphoreType.DMA((4, 2)),
    m_ss=pltpu.SemaphoreType.DMA((2,)),
    m_rs=pltpu.SemaphoreType.DMA((2,)),
    y_ss=pltpu.SemaphoreType.DMA((8,)),
    y_rs=pltpu.SemaphoreType.DMA((8,)),
    f_ss=pltpu.SemaphoreType.DMA,
    f_rs=pltpu.SemaphoreType.DMA,
)
OWN = 7


def swap_parts(v):
    lane = lax.rem(iota(v.shape, 1), 64)
    return jnp.where(lane < 32, pltpu.roll(v, 96, 1), pltpu.roll(v, 32, 1))


def turned(a, r, block, gain, g):
    v = block.astype(F32)
    v = v * lax.rsqrt(jnp.mean(v * v, axis=1, keepdims=True) + EPS) * gain
    at = a.ep * (ROWS // GRID) + g
    cos = r.rowcs[0, pl.ds(at, 1), :] + r.colcs[0]
    sin = r.rowcs[1, pl.ds(at, 1), :] + r.colcs[1]
    return (v * cos + swap_parts(v) * sin).astype(BF16)


def column_half(r, half):
    return r.wo_h.at[:, pl.ds(pl.multiple_of(half * 1024, 1024), 1024)]


def own_columns(a, r):
    return pltpu.make_async_copy(column_half(r, a.c), r.wo.at[a.c], r.wo_sem)


def partner_columns(a, r):
    return remote(column_half(r, 1 - a.c), r.wo.at[a.c], r.we_ss, r.we_rs, c=1 - a.c)


def mix_turn(a, r):
    own_columns(a, r).start()
    keys = []
    for g in range(ROWS // GRID):
        at = slice(g * GRID, g * GRID + GRID)
        for h in range(2):
            q = turned(a, r, r.q_in[at, h * 128 : h * 128 + 128], r.qg[...] * SCALE, g)
            r.q_all[0, h * ROWS + g * GRID : h * ROWS + g * GRID + GRID, :] = q
        keys.append(turned(a, r, r.k_in[at, :], r.kg[...], g))
    key = jnp.concatenate(keys, axis=0)
    r.kt[OWN] = key.astype(F32).T.astype(BF16)
    r.va[OWN] = r.v_in[...]
    r.vx[:, :, 128:] = jnp.ones((2, 2 * ROWS, 128), BF16)
    r.mx[...] = jnp.full(r.mx.shape, -1e30, F32)
    r.acc[...] = jnp.zeros(r.acc.shape, F32)


def q_copy(a, r, d):
    return remote(r.q_all.at[0], r.q_all.at[NX - d], r.xq_ss.at[d], r.xq_rs.at[d], x=around(a.x, d, NX))


def kv_copy(a, r, slot, part):
    src = OWN if slot < 2 else slot - 2
    z = around(a.z, 1 if slot % 2 == 0 else -1, NZ)
    buf, ss, rs = ((r.kt, r.k_ss, r.k_rs), (r.va, r.v_ss, r.v_rs))[part]
    return remote(buf.at[src], buf.at[slot], ss.at[slot], rs.at[slot], z=z)


def kv_start(a, r, slot, part):
    kv_copy(a, r, slot, part).start()


def kv_arrived(a, r, slots):
    for part in range(2):
        for slot in slots:
            kv_copy(a, r, slot, part).wait_recv()
            if slot + 2 < OWN:
                kv_start(a, r, slot + 2, part)


def mix_send(a, r):
    for part in range(2):
        kv_start(a, r, 0, part)
        kv_start(a, r, 1, part)
    for d in (2, 1, 3):
        q_copy(a, r, d).start()


def attend_rows(r, s, xs, at):
    q = r.q_all[xs, at, :]
    even = s % 2
    s = jnp.dot(q, r.kx[even], preferred_element_type=F32)
    old = r.mx[xs, at, :]
    new = jnp.maximum(old, jnp.max(s, axis=1, keepdims=True))
    r.mx[xs, at, :] = new
    p = jnp.concatenate(
        [jnp.exp2(s[:, j * 128 : j * 128 + 128] - new).astype(BF16) for j in range(6)], axis=1
    )
    keep = jnp.exp2(old - new)
    pv = jnp.dot(p, r.vx[even], preferred_element_type=F32)
    acc = r.acc[xs, at, :]
    r.acc[xs, at, :] = acc * jnp.concatenate([keep, keep], axis=1) + pv


TILE = 128


def mix_arrived(a, r, s):
    kv_arrived(a, r, [slot for slot in (2 * s, 2 * s + 1) if slot != OWN])


def mix_keys(r, s):
    for i in range(2):
        r.kx[s % 2, :, i * ROWS : i * ROWS + ROWS] = r.kt[2 * s + i]
        r.vx[s % 2, i * ROWS : i * ROWS + ROWS, :128] = r.va[2 * s + i]


def mix_rows(r, s, targets):
    for xs in targets:
        for t in range(2 * ROWS // TILE):
            attend_rows(r, s, xs, slice(t * TILE, t * TILE + TILE))


def part_copies(a, r, d, h):
    x = around(a.x, d, NX)
    return (
        remote(r.ob.at[d, h], r.orc.at[d, h], r.o_ss.at[d, h], r.o_rs.at[d, h], x=x),
        remote(r.lb.at[d, h], r.lrc.at[d, h], r.l_ss.at[d, h], r.l_rs.at[d, h], x=x),
    )


def mix_last_rows(a, r, d):
    xs = d
    dst_o, dst_l = (r.ob, r.lb) if d else (r.orc, r.lrc)
    for h in range(2):
        for t in range(ROWS // TILE):
            at = slice(h * ROWS + t * TILE, h * ROWS + t * TILE + TILE)
            attend_rows(r, 3, xs, at)
            acc = r.acc[xs, at, :]
            total = acc[:, 128:]
            dst_o[d, h, t * TILE : t * TILE + TILE, :] = (acc[:, :128] / total).astype(BF16)
            dst_l[d, h, t : t + 1, :] = to_row(r.mx[xs, at, :] + jnp.log2(total))
        if d:
            for cp in part_copies(a, r, d, h):
                cp.start()


def mix_heads_copy(a, r, h):
    mine = r.att.at[a.c, h]
    return remote(mine, mine, r.m_ss.at[h], r.m_rs.at[h], c=1 - a.c)


def mix_combine(a, r):
    for h in range(2):
        for d in (2, 1, 3):
            for cp in part_copies(a, r, d, h):
                cp.wait_recv()
        for t in range(3):
            lse = [to_col(r.lrc[d, h, t : t + 1, :]) for d in range(NX)]
            top = functools.reduce(jnp.maximum, lse)
            w = [jnp.exp2(v - top) for v in lse]
            inv = 1.0 / functools.reduce(jnp.add, w)
            at = slice(t * 128, t * 128 + 128)
            o = None
            for d in range(NX):
                term = r.orc[d, h, at, :].astype(F32) * (w[d] * inv)
                o = term if o is None else o + term
            r.att[a.c, h, at, :] = o.astype(BF16)
        mix_heads_copy(a, r, h).start()


def project(r, core, j):
    rows = jnp.concatenate([r.att[core, 0], r.att[core, 1]], axis=1)
    return jnp.dot(rows, r.wo[core, :, j * 256 : j * 256 + 256], preferred_element_type=F32)


def mix_project(a, r):
    own_columns(a, r).wait()
    for j in range(4):
        r.mp[:, j * 256 : j * 256 + 256] = project(r, a.c, j)
    partner_columns(a, r).wait_recv()
    for h in range(2):
        mix_heads_copy(a, r, h).wait_recv()
    for j in range(4):
        r.mp[:, j * 256 : j * 256 + 256] += project(r, 1 - a.c, j)


def mix_tree_copy(a, r, role):
    return tree_copy(a, r.ms, r.yl, r.yr, r.y_ss, r.y_rs, role)


def mix_pair_total(a, r, i):
    y = around(a.y, PAIR_ORDER[i], NY)
    at = pl.ds(pl.multiple_of(y * 48, 16), 48)
    return y, r.mp[at, :]


def mix_scatter(a, r):
    for role in range(5):
        y, total = mix_pair_total(a, r, role)
        r.ms[y] = total.astype(BF16)
        mix_tree_copy(a, r, role).start()
    r.fs[...] = mix_pair_total(a, r, 7)[1]


def mix_relay(a, r):
    mix_tree_copy(a, r, 2).wait_recv()
    for role in (5, 6):
        y, total = mix_pair_total(a, r, role)
        mix_tree_copy(a, r, role - 5).wait_recv()
        r.ms[y] = (total + relayed(a, r.yl, role)).astype(BF16)
        mix_tree_copy(a, r, role).start()


def mix_final_copy(a, r):
    src = r.fs.at[pl.ds(pl.multiple_of((1 - a.c) * 24, 8), 24)]
    return remote(src, r.fr, r.f_ss, r.f_rs, c=1 - a.c)


def mix_sum(a, r):
    total = r.fs[...]
    for role in range(3, 7):
        mix_tree_copy(a, r, role).wait_recv()
        total = total + r.yr[role - 3].astype(F32)
    r.fs[...] = total
    mix_final_copy(a, r).start()


def mix_finish(a, r, out):
    mix_final_copy(a, r).wait()
    mine = r.fs[pl.ds(pl.multiple_of(a.c * 24, 8), 24), :]
    other = r.fr[...]
    sq = jnp.sum(mine * mine, axis=1, keepdims=True) + jnp.sum(other * other, axis=1, keepdims=True)
    inv = lax.rsqrt(sq * (1.0 / D) + EPS)
    for half, v in ((a.c, mine), (1 - a.c, other)):
        off = pl.ds(pl.multiple_of(half * 1024, 1024), 1024)
        out[:, off] = (v * inv * r.mgain[:, off]).astype(BF16)
    for d in (1, 2, 3):
        q_copy(a, r, d).wait_send()
        for h in range(2):
            for cp in part_copies(a, r, d, h):
                cp.wait_send()
    for slot in range(OWN):
        for part in range(2):
            kv_copy(a, r, slot, part).wait_send()
    partner_columns(a, r).wait_send()
    for h in range(2):
        mix_heads_copy(a, r, h).wait_send()
    for role in range(7):
        mix_tree_copy(a, r, role).wait_send()


def bind(names, refs):
    return SimpleNamespace(**dict(zip(names, refs, strict=True)))


def kernel(*refs):
    r = bind((*MOE_IN[:-3], *MIX_IN[:-1], *MOE_IN[-3:], MIX_IN[-1], "moe_out", "mix_out", *SCRATCH), refs)
    a = here()
    r.drecv[...] = jnp.zeros(r.drecv.shape, BF16)
    r.rrecv[...] = jnp.zeros(r.rrecv.shape, BF16)
    barrier = pltpu.get_barrier_semaphore()
    greet_ep(a, barrier)
    greet_tp(a, barrier)
    moe_weights(r)
    moe_dispatch_build(a, r)
    mix_turn(a, r)
    pl.semaphore_wait(barrier, 46)
    exchange_start(a, r.disp, r.drecv, r.d_ss, r.d_rs)
    mix_send(a, r)
    partner_columns(a, r).start()
    exchange_wait(r.disp, r.drecv, r.d_ss, r.d_rs)
    moe_compact(a, r)
    moe_gather_start(a, r)
    mix_arrived(a, r, 0)
    mix_keys(r, 0)
    mix_rows(r, 0, (0,))
    for d in (1, 2, 3):
        q_copy(a, r, d).wait_recv()
    mix_rows(r, 0, (1, 2, 3))
    moe_gather_forward(a, r, 0)
    mix_arrived(a, r, 1)
    mix_keys(r, 1)
    mix_rows(r, 1, (0,))
    moe_experts(a, r, 0)
    moe_gather_forward(a, r, 1)
    mix_rows(r, 1, (1,))
    moe_pair_sums(a, r, 0)
    moe_experts(a, r, 1)
    mix_rows(r, 1, (2,))
    moe_pair_sums(a, r, 1)
    moe_gather_forward(a, r, 2)
    mix_arrived(a, r, 2)
    mix_rows(r, 1, (3,))
    moe_experts(a, r, 2)
    mix_keys(r, 2)
    mix_rows(r, 2, (2,))
    moe_pair_sums(a, r, 2)
    moe_relay(a, r, 0)
    mix_rows(r, 2, (1, 3))
    moe_relay(a, r, 1)
    mix_arrived(a, r, 3)
    mix_keys(r, 3)
    mix_last_rows(a, r, 2)
    mix_last_rows(a, r, 1)
    mix_rows(r, 2, (0,))
    moe_relay(a, r, 2)
    mix_last_rows(a, r, 3)
    mix_last_rows(a, r, 0)
    moe_return_start(a, r)
    mix_combine(a, r)
    mix_project(a, r)
    moe_combine(a, r)
    mix_scatter(a, r)
    moe_finish(a, r, r.moe_out)
    mix_relay(a, r)
    mix_sum(a, r)
    mix_finish(a, r, r.mix_out)


SCRATCH = MOE_SCRATCH | MIX_SCRATCH


def call(ins, hbm):
    n = len(ins) - hbm
    return pl.pallas_call(
        kernel,
        out_shape=(jax.ShapeDtypeStruct((TOKENS2, 128), BF16), jax.ShapeDtypeStruct((24, D), BF16)),
        in_specs=[pl.BlockSpec(memory_space=pltpu.VMEM)] * n + [pl.BlockSpec(memory_space=pl.ANY)] * hbm,
        out_specs=(pl.BlockSpec(memory_space=pltpu.VMEM),) * 2,
        scratch_shapes=list(SCRATCH.values()),
        compiler_params=pltpu.CompilerParams(
            collective_id=0, has_side_effects=True, vmem_limit_bytes=60 * 2**20
        ),
        cost_estimate=pl.CostEstimate(flops=10**10, bytes_accessed=2**23, transcendentals=0),
    )(*ins)


def turn_tables():
    freq = (THETA ** (-np.arange(0, 64, 2, dtype=np.float32) / np.float32(64))).astype(np.float32)
    row = np.arange(192, dtype=np.float32)[:, None] * freq[None]
    col = np.arange(64, dtype=np.float32)[:, None] * freq[None]
    rowcs = np.zeros((2, 192, 128), np.float32)
    colcs = np.zeros((2, 64, 128), np.float32)
    rowcs[0, :, 0:32] = rowcs[0, :, 32:64] = np.cos(row)
    rowcs[1, :, 0:32], rowcs[1, :, 32:64] = -np.sin(row), np.sin(row)
    colcs[0, :, 64:96] = colcs[0, :, 96:128] = np.cos(col)
    colcs[1, :, 64:96], colcs[1, :, 96:128] = -np.sin(col), np.sin(col)
    return jnp.asarray(rowcs), jnp.asarray(colcs)


def per_device(
    query_rows,
    key_rows,
    value_rows,
    query_gain,
    key_gain,
    w_out,
    mixer_gain,
    expert_input,
    expert_ids,
    expert_weights,
    input_gain,
    w_gate,
    w_up,
    w_down,
    out_gain,
):
    rowcs, colcs = turn_tables()
    moe, mix = call(
        (
            expert_input,
            expert_ids.T,
            expert_weights.T,
            input_gain.reshape(1, D),
            out_gain.reshape(1, 128),
            query_rows,
            key_rows,
            value_rows,
            query_gain.reshape(1, HEAD),
            key_gain.reshape(1, HEAD),
            rowcs,
            colcs,
            mixer_gain.reshape(1, D),
            w_gate[0],
            w_up[0],
            w_down[0],
            w_out,
        ),
        4,
    )
    return (mix, moe)


def solution(mesh):
    finer = Mesh(mesh.devices.reshape(NZ, NX, NY, NC), ("z", "x", "y", "c"))
    in_specs = (
        P(EP, TP),
        P(EP, TP),
        P(EP, TP),
        P(),
        P(),
        P(TP, None),
        P(),
        P(EP, None),
        P(EP, None),
        P(EP, None),
        P(),
        P(EP, None, TP),
        P(EP, None, TP),
        P(EP, TP, None),
        P(TP),
    )
    out_specs = (P(EP + TP, None), P(EP, TP))
    return jax.shard_map(
        per_device, mesh=finer, in_specs=in_specs, out_specs=out_specs, check_vma=False
    )
```

```python
import functools
from types import SimpleNamespace

import numpy as np
import jax
import jax.numpy as jnp
from jax import lax
from jax.experimental import pallas as pl
from jax.experimental.pallas import tpu as pltpu
from jax.sharding import Mesh
from jax.sharding import PartitionSpec as P

NZ, NX, NY, NC = 8, 4, 8, 2
EP = ("z", "x")
TP = ("y", "c")
D = 2048
HEAD = 128
GRID = 64
ROWS = 384
TOKENS2 = 192
CAP = 18
SLAB = 32
EXPERTS = 32
SLOTS = EXPERTS * CAP
PADDED = EXPERTS * SLAB
EPS = 1e-06
SCALE = float(np.log2(np.e) * HEAD**-0.5)
THETA = 10000.0
F32 = jnp.float32
BF16 = jnp.bfloat16
MESH_ID = pl.DeviceIdType.MESH
PAIR_ORDER = (3, -3, 4, 1, -1, 2, -2, 0)
ROLE_TO = (1, -1, 0, 1, -1, 2, -2)
SENT = 24
BLOCKS = 3
BLOCK = 192
X_ORDER = (2, 1, 3, 0)


def around(i, d, n):
    return lax.rem(i + (d % n), n)


def here():
    a = SimpleNamespace()
    a.z, a.x, a.y, a.c = (lax.axis_index(n) for n in ("z", "x", "y", "c"))
    a.ep = a.z * NX + a.x
    return a


def remote(src, dst, ss, rs, **dev):
    return pltpu.make_async_remote_copy(
        src_ref=src, dst_ref=dst, send_sem=ss, recv_sem=rs, device_id=dev, device_id_type=MESH_ID
    )


def ep_peer(a, k):
    e = lax.rem(a.ep + k, EXPERTS)
    return e, lax.div(e, NX), lax.rem(e, NX)


def greet_ep(a, barrier):
    def one(k, carry):
        _, z, x = ep_peer(a, k)
        pl.semaphore_signal(barrier, inc=1, device_id={"z": z, "x": x}, device_id_type=MESH_ID)
        return carry

    lax.fori_loop(1, EXPERTS, one, 0)


def greet_tp(a, barrier):
    for d in range(NY):
        for o in range(2):
            if d or o:
                c = a.c if o == 0 else 1 - a.c
                pl.semaphore_signal(
                    barrier, inc=1, device_id={"y": around(a.y, d, NY), "c": c}, device_id_type=MESH_ID
                )


def wait_bytes(ref, sem):
    pltpu.make_async_copy(ref, ref, sem).wait()


def iota(shape, dim):
    return lax.broadcasted_iota(jnp.int32, shape, dim)


def eye128():
    return iota((128, 128), 0) == iota((128, 128), 1)


def to_row(col):
    return jnp.sum(jnp.where(eye128(), col, 0.0), axis=0, keepdims=True)


def to_col(row):
    return jnp.sum(jnp.where(eye128(), row, 0.0), axis=1, keepdims=True)


def tree_copy(a, src, relay, final, ss, rs, role, at=()):
    to = around(a.y, ROLE_TO[role], NY) if role != 2 else lax.rem(a.y + 2 + 4 * a.c, NY)
    dst = relay.at[(role, *at)] if role < 3 else final.at[(role - 3, *at)]
    mine = src.at[(around(a.y, PAIR_ORDER[role], NY), *at)]
    return remote(mine, dst, ss.at[(*at, role)], rs.at[(*at, role)], y=to)


def relayed(a, relay, role, at=()):
    share = jnp.where(a.c == 0, 1.0, 0.0) if role == 5 else jnp.where(a.c == 0, 0.0, 1.0)
    return relay[(role - 5, *at)].astype(F32) + relay[(2, *at)].astype(F32) * share


MOE_IN = ("xin", "ids", "wts", "igain", "ogain", "wg_h", "wu_h", "wd_h")
MOE_SCRATCH = dict(
    disp=pltpu.VMEM((EXPERTS, SLAB, 256), BF16),
    drecv=pltpu.VMEM((EXPERTS, SLAB, 256), BF16),
    xg=pltpu.VMEM((2, 4, BLOCKS, 2, BLOCK, 128), BF16),
    xcat=pltpu.VMEM((BLOCK, D), BF16),
    wg=pltpu.VMEM((D, 256), BF16),
    wu=pltpu.VMEM((D, 256), BF16),
    wd=pltpu.VMEM((256, D), BF16),
    part=pltpu.VMEM((2, NY, BLOCKS, BLOCK, 128), BF16),
    pr=pltpu.VMEM((NY, BLOCKS, BLOCK, 128), BF16),
    ps=pltpu.VMEM((NY, BLOCKS, BLOCK, 128), BF16),
    own=pltpu.VMEM((BLOCKS, BLOCK, 128), F32),
    rs=pltpu.VMEM((4, BLOCKS, BLOCK, 128), BF16),
    rl=pltpu.VMEM((3, BLOCKS, BLOCK, 128), BF16),
    rsend=pltpu.VMEM((EXPERTS, SLAB, 128), BF16),
    rrecv=pltpu.VMEM((EXPERTS, SLAB, 128), BF16),
    comb=pltpu.VMEM((TOKENS2, 128), F32),
    scol=pltpu.VMEM((TOKENS2, 2), jnp.int32),
    sqs=pltpu.VMEM((8, 128), F32),
    sqr=pltpu.VMEM((16, 8, 128), F32),
    w_sem=pltpu.SemaphoreType.DMA((3,)),
    d_ss=pltpu.SemaphoreType.DMA,
    d_rs=pltpu.SemaphoreType.DMA,
    ag_ss=pltpu.SemaphoreType.DMA((BLOCKS, 3)),
    ag_rs=pltpu.SemaphoreType.DMA((BLOCKS, 3)),
    pf_ss=pltpu.SemaphoreType.DMA((BLOCKS, 4)),
    pf_rs=pltpu.SemaphoreType.DMA((BLOCKS, 4)),
    pp_ss=pltpu.SemaphoreType.DMA((BLOCKS, 8)),
    pp_rs=pltpu.SemaphoreType.DMA((BLOCKS, 8)),
    rs_ss=pltpu.SemaphoreType.DMA((BLOCKS, 8)),
    rs_rs=pltpu.SemaphoreType.DMA((BLOCKS, 8)),
    t_ss=pltpu.SemaphoreType.DMA,
    t_rs=pltpu.SemaphoreType.DMA,
    q_ss=pltpu.SemaphoreType.DMA,
    q_rs=pltpu.SemaphoreType.DMA,
)


def moe_weights(r):
    for i, (src, dst) in enumerate(((r.wg_h, r.wg), (r.wu_h, r.wu), (r.wd_h, r.wd))):
        pltpu.make_async_copy(src, dst, r.w_sem.at[i]).start()


def moe_weights_wait(r):
    for i, (src, dst) in enumerate(((r.wg_h, r.wg), (r.wu_h, r.wu), (r.wd_h, r.wd))):
        pltpu.make_async_copy(src, dst, r.w_sem.at[i]).wait()


def to_cols(row):
    return jnp.concatenate([to_col(row[:, :128]), to_col(row[:, 64:])[64:]], axis=0)


def moe_slots(r):
    rows = [r.ids[k : k + 1, :].astype(F32) for k in range(2)]
    cols = [to_cols(v) for v in rows]
    shape = (TOKENS2, TOKENS2)
    above, left = iota(shape, 0) < iota(shape, 1), iota(shape, 1) < iota(shape, 0)

    def rank(here, there, mask, dim):
        hits = [jnp.where((here == v) & mask, 1.0, 0.0) for v in there]
        return here * SLAB + jnp.sum(hits[0] + hits[1], axis=dim, keepdims=True)

    srow = [rank(v, cols, above, 0).astype(jnp.int32) for v in rows]
    scol = [rank(v, rows, left, 1).astype(jnp.int32) for v in cols]
    return srow, scol


def moe_dispatch_build(a, r):
    srow, scol = moe_slots(r)
    r.scol[...] = jnp.concatenate(scol, axis=1)
    x = r.xin[...].astype(F32)
    inv = lax.rsqrt(jnp.sum(x * x, axis=1, keepdims=True) * (1.0 / D) + EPS)
    g = lax.rem(a.y, 4)
    halves = []
    for j in range(2):
        off = pl.multiple_of(((g + 4 * j) * 2 + a.c) * 128, 128)
        xs = r.xin[:, pl.ds(off, 128)].astype(F32)
        halves.append((xs * inv * r.igain[:, pl.ds(off, 128)]).astype(BF16))
    nn = jnp.concatenate(halves, axis=1)
    rows = iota((PADDED, TOKENS2), 0)
    pick = (rows == srow[0]) | (rows == srow[1])
    pick = jnp.where(pick, 1.0, 0.0).astype(BF16)
    out = jnp.dot(pick, nn, preferred_element_type=F32).astype(BF16)
    r.disp[...] = out.reshape(EXPERTS, SLAB, 256)


def head(ref, e):
    return ref.at[e, pl.ds(0, SENT)]


def exchange_start(a, src, dst, ss, rs):
    def one(k, carry):
        e, z, x = ep_peer(a, k)
        remote(head(src, e), head(dst, a.ep), ss, rs, z=z, x=x).start()
        return carry

    lax.fori_loop(1, EXPERTS, one, 0)
    dst[a.ep] = src[a.ep]


def exchange_wait(src, dst, ss, rs):
    wait_bytes(dst.at[pl.ds(0, EXPERTS - 1), pl.ds(0, SENT)], rs)
    wait_bytes(src.at[pl.ds(0, EXPERTS - 1), pl.ds(0, SENT)], ss)


def padded_place(i):
    e = ((i.astype(F32) + 0.5) * (1.0 / CAP)).astype(jnp.int32)
    return i + e * (SLAB - CAP)


def moe_compact(a, r):
    g = lax.rem(a.y, 4)
    place = padded_place(iota((SLOTS, 1), 0))
    pick = jnp.where(iota((SLOTS, PADDED), 1) == place, 1.0, 0.0).astype(BF16)
    got = r.drecv[...].reshape(PADDED, 256)
    out = jnp.dot(pick, got, preferred_element_type=F32).astype(BF16)
    for b in range(BLOCKS):
        for h in range(2):
            r.xg[a.c, g, b, h] = out[b * BLOCK : b * BLOCK + BLOCK, h * 128 : h * 128 + 128]


def moe_gather_copy(a, r, b, i):
    src = r.xg.at[a.c, lax.rem(a.y, 4), b]
    to = around(a.y, (1, -1)[i], NY) if i < 2 else lax.rem(a.y + 2 + 4 * a.c, NY)
    return remote(src, src, r.ag_ss.at[b, i], r.ag_rs.at[b, i], y=to)


def moe_group(a, i):
    return around(lax.rem(a.y, 4), (0, 3, 1, 2)[i], 4)


def moe_partner_copy(a, r, b, i):
    src = r.xg.at[a.c, moe_group(a, i), b]
    return remote(src, src, r.pf_ss.at[b, i], r.pf_rs.at[b, i], c=1 - a.c)


def moe_gather_start(a, r):
    for b in range(BLOCKS):
        for i in (2, 0, 1):
            moe_gather_copy(a, r, b, i).start()
    for b in range(BLOCKS):
        moe_partner_copy(a, r, b, 0).start()


def moe_gather_forward(a, r, b):
    for i in range(3):
        moe_gather_copy(a, r, b, i).wait_recv()
        moe_partner_copy(a, r, b, i + 1).start()


def moe_experts(a, r, b):
    for i in range(4):
        moe_partner_copy(a, r, b, i).wait_recv()
    for par in range(2):
        for g in range(4):
            for h in range(2):
                at = ((g + 4 * h) * 2 + par) * 128
                r.xcat[:, at : at + 128] = r.xg[par, g, b, h]
    if b == 0:
        moe_weights_wait(r)
    xb = r.xcat[...]
    gate = jnp.dot(xb, r.wg[...], preferred_element_type=F32)
    up = jnp.dot(xb, r.wu[...], preferred_element_type=F32)
    hid = (gate / (1.0 + jnp.exp(-gate)) * up).astype(BF16)
    for ys in range(NY):
        o = jnp.dot(hid, r.wd[:, ys * 256 : ys * 256 + 256], preferred_element_type=F32)
        o = o.astype(BF16)
        r.part[0, ys, b] = o[:, :128]
        r.part[1, ys, b] = o[:, 128:]
    for i in range(NY):
        moe_pair_copy(a, r, b, i).start()


def moe_pair_copy(a, r, b, i):
    ys = around(a.y, PAIR_ORDER[i], NY)
    return remote(r.part.at[1 - a.c, ys, b], r.pr.at[ys, b], r.pp_ss.at[b, i], r.pp_rs.at[b, i], c=1 - a.c)


def moe_tree_copy(a, r, b, role):
    return tree_copy(a, r.ps, r.rl, r.rs, r.rs_ss, r.rs_rs, role, (b,))


def moe_pair_total(a, r, b, i):
    ys = around(a.y, PAIR_ORDER[i], NY)
    moe_pair_copy(a, r, b, i).wait_recv()
    return ys, r.part[a.c, ys, b].astype(F32) + r.pr[ys, b].astype(F32)


def moe_pair_sums(a, r, b):
    for role in range(5):
        ys, total = moe_pair_total(a, r, b, role)
        r.ps[ys, b] = total.astype(BF16)
        moe_tree_copy(a, r, b, role).start()
    r.own[b] = moe_pair_total(a, r, b, 7)[1]


def moe_relay(a, r, b):
    moe_tree_copy(a, r, b, 2).wait_recv()
    for role in (5, 6):
        ys, total = moe_pair_total(a, r, b, role)
        moe_tree_copy(a, r, b, role - 5).wait_recv()
        r.ps[ys, b] = (total + relayed(a, r.rl, role, (b,))).astype(BF16)
        moe_tree_copy(a, r, b, role).start()


def moe_return_start(a, r):
    rows = []
    for b in range(BLOCKS):
        total = r.own[b]
        for role in range(3, 7):
            moe_tree_copy(a, r, b, role).wait_recv()
            total = total + r.rs[role - 3, b].astype(F32)
        rows.append(total.astype(BF16))
    rows = jnp.concatenate(rows, axis=0)
    place = padded_place(iota((1, SLOTS), 1))
    pick = jnp.where(iota((PADDED, SLOTS), 0) == place, 1.0, 0.0).astype(BF16)
    out = jnp.dot(pick, rows, preferred_element_type=F32).astype(BF16)
    r.rsend[...] = out.reshape(EXPERTS, SLAB, 128)
    exchange_start(a, r.rsend, r.rrecv, r.t_ss, r.t_rs)


def square_targets(a):
    out = []
    for d in range(NY):
        for o in range(2):
            if d or o:
                out.append((around(a.y, d, NY), a.c if o == 0 else 1 - a.c))
    return out


def moe_combine(a, r):
    exchange_wait(r.rsend, r.rrecv, r.t_ss, r.t_rs)
    got = r.rrecv[...].reshape(PADDED, 128)
    total = None
    for k in range(2):
        pick = jnp.where(iota((TOKENS2, PADDED), 1) == r.scol[:, k : k + 1], 1.0, 0.0).astype(BF16)
        term = jnp.dot(pick, got, preferred_element_type=F32) * to_cols(r.wts[k : k + 1, :])
        total = term if total is None else total + term
    r.comb[...] = total
    sq = jnp.sum(total * total, axis=1, keepdims=True)
    r.sqs[...] = jnp.zeros((8, 128), F32)
    r.sqs[0:1, :] = to_row(sq[:128])
    r.sqs[1:2, :] = to_row(sq[64:])
    tp = a.y * 2 + a.c
    for y, c in square_targets(a):
        remote(r.sqs, r.sqr.at[tp], r.q_ss, r.q_rs, y=y, c=c).start()
    r.sqr[tp] = r.sqs[...]


def moe_finish(a, r, out):
    wait_bytes(r.sqr.at[pl.ds(0, 15)], r.q_rs)
    wait_bytes(r.sqr.at[pl.ds(0, 15)], r.q_ss)
    tot = r.sqr[0]
    for i in range(1, 16):
        tot = tot + r.sqr[i]
    inv = lax.rsqrt(tot * (1.0 / D) + EPS)
    lo, hi = to_col(inv[0:1, :]), to_col(inv[1:2, :])
    out[0:128, :] = (r.comb[0:128, :] * lo * r.ogain[...]).astype(BF16)
    out[128:192, :] = (r.comb[128:192, :] * hi[64:] * r.ogain[...]).astype(BF16)
    for b in range(BLOCKS):
        for i in range(3):
            moe_gather_copy(a, r, b, i).wait_send()
        for i in range(4):
            moe_partner_copy(a, r, b, i).wait_send()
        for role in range(7):
            moe_tree_copy(a, r, b, role).wait_send()
        for i in range(NY):
            moe_pair_copy(a, r, b, i).wait_send()


MIX_IN = ("q_in", "k_in", "v_in", "qg", "kg", "rowcs", "colcs", "mgain", "wo_h")
MIX_SCRATCH = dict(
    q_all=pltpu.VMEM((NX, 2 * ROWS, HEAD), BF16),
    kt=pltpu.VMEM((NZ, HEAD, ROWS), BF16),
    va=pltpu.VMEM((NZ, ROWS, HEAD), BF16),
    kx=pltpu.VMEM((HEAD, 2 * ROWS), BF16),
    vx=pltpu.VMEM((2 * ROWS, 256), BF16),
    mx=pltpu.VMEM((NX, 2 * ROWS, 128), F32),
    acc=pltpu.VMEM((NX, 2 * ROWS, 256), F32),
    ob=pltpu.VMEM((NX, 2 * ROWS, HEAD), BF16),
    lb=pltpu.VMEM((NX, 8, 128), F32),
    orc=pltpu.VMEM((NX, 2 * ROWS, HEAD), BF16),
    lrc=pltpu.VMEM((NX, 8, 128), F32),
    att=pltpu.VMEM((ROWS, 256), BF16),
    wo=pltpu.VMEM((256, D), BF16),
    mp=pltpu.VMEM((2, ROWS, 1024), BF16),
    mr=pltpu.VMEM((ROWS, 1024), BF16),
    ms=pltpu.VMEM((NY, 48, 1024), BF16),
    yr=pltpu.VMEM((4, 48, 1024), BF16),
    yl=pltpu.VMEM((3, 48, 1024), BF16),
    fs=pltpu.VMEM((48, 1024), F32),
    fr=pltpu.VMEM((24, 1024), F32),
    wo_sem=pltpu.SemaphoreType.DMA,
    xq_ss=pltpu.SemaphoreType.DMA((4,)),
    xq_rs=pltpu.SemaphoreType.DMA((4,)),
    k_ss=pltpu.SemaphoreType.DMA((8,)),
    k_rs=pltpu.SemaphoreType.DMA((8,)),
    v_ss=pltpu.SemaphoreType.DMA((8,)),
    v_rs=pltpu.SemaphoreType.DMA((8,)),
    o_ss=pltpu.SemaphoreType.DMA((4,)),
    o_rs=pltpu.SemaphoreType.DMA((4,)),
    l_ss=pltpu.SemaphoreType.DMA((4,)),
    l_rs=pltpu.SemaphoreType.DMA((4,)),
    m_ss=pltpu.SemaphoreType.DMA((2,)),
    m_rs=pltpu.SemaphoreType.DMA((2,)),
    y_ss=pltpu.SemaphoreType.DMA((8,)),
    y_rs=pltpu.SemaphoreType.DMA((8,)),
    f_ss=pltpu.SemaphoreType.DMA,
    f_rs=pltpu.SemaphoreType.DMA,
)
OWN = 7


def swap_parts(v):
    lane = lax.rem(iota(v.shape, 1), 64)
    return jnp.where(lane < 32, pltpu.roll(v, 96, 1), pltpu.roll(v, 32, 1))


def turned(a, r, block, gain, g):
    v = block.astype(F32)
    v = v * lax.rsqrt(jnp.mean(v * v, axis=1, keepdims=True) + EPS) * gain
    at = a.ep * (ROWS // GRID) + g
    cos = r.rowcs[0, pl.ds(at, 1), :] + r.colcs[0]
    sin = r.rowcs[1, pl.ds(at, 1), :] + r.colcs[1]
    return (v * cos + swap_parts(v) * sin).astype(BF16)


def mix_turn(a, r):
    pltpu.make_async_copy(r.wo_h, r.wo, r.wo_sem).start()
    keys = []
    for g in range(ROWS // GRID):
        at = slice(g * GRID, g * GRID + GRID)
        for h in range(2):
            q = turned(a, r, r.q_in[at, h * 128 : h * 128 + 128], r.qg[...] * SCALE, g)
            r.q_all[a.x, h * ROWS + g * GRID : h * ROWS + g * GRID + GRID, :] = q
        keys.append(turned(a, r, r.k_in[at, :], r.kg[...], g))
    key = jnp.concatenate(keys, axis=0)
    r.kt[OWN] = key.astype(F32).T.astype(BF16)
    r.va[OWN] = r.v_in[...]
    r.vx[:, 128:] = jnp.ones((2 * ROWS, 128), BF16)
    r.mx[...] = jnp.full(r.mx.shape, -1e30, F32)
    r.acc[...] = jnp.zeros(r.acc.shape, F32)


def q_copy(a, r, d):
    mine = r.q_all.at[a.x]
    return remote(mine, mine, r.xq_ss.at[d], r.xq_rs.at[d], x=around(a.x, d, NX))


def kv_copies(a, r, slot):
    src = OWN if slot < 2 else slot - 2
    z = around(a.z, 1 if slot % 2 == 0 else -1, NZ)
    return (
        remote(r.kt.at[src], r.kt.at[slot], r.k_ss.at[slot], r.k_rs.at[slot], z=z),
        remote(r.va.at[src], r.va.at[slot], r.v_ss.at[slot], r.v_rs.at[slot], z=z),
    )


def kv_start(a, r, slot):
    for cp in kv_copies(a, r, slot):
        cp.start()


def kv_arrived(a, r, slots):
    for part in range(2):
        for slot in slots:
            kv_copies(a, r, slot)[part].wait_recv()
            if slot + 2 < OWN:
                kv_copies(a, r, slot + 2)[part].start()


def mix_send(a, r):
    kv_start(a, r, 0)
    kv_start(a, r, 1)
    for d in (2, 1, 3):
        q_copy(a, r, d).start()


def attend_rows(r, xs, at):
    q = r.q_all[xs, at, :]
    s = jnp.dot(q, r.kx[...], preferred_element_type=F32)
    old = r.mx[xs, at, :]
    new = jnp.maximum(old, jnp.max(s, axis=1, keepdims=True))
    r.mx[xs, at, :] = new
    p = jnp.concatenate(
        [jnp.exp2(s[:, j * 128 : j * 128 + 128] - new).astype(BF16) for j in range(6)], axis=1
    )
    keep = jnp.exp2(old - new)
    pv = jnp.dot(p, r.vx[...], preferred_element_type=F32)
    acc = r.acc[xs, at, :]
    r.acc[xs, at, :] = acc * jnp.concatenate([keep, keep], axis=1) + pv


TILE = 256


def mix_step(a, r, s):
    slots = (2 * s, 2 * s + 1)
    kv_arrived(a, r, [slot for slot in slots if slot != OWN])
    for i, slot in enumerate(slots):
        r.kx[:, i * ROWS : i * ROWS + ROWS] = r.kt[slot]
        r.vx[i * ROWS : i * ROWS + ROWS, :128] = r.va[slot]


def mix_rows(r, lo, hi):
    def one(xs, carry):
        for t in range(2 * ROWS // TILE):
            attend_rows(r, xs, slice(t * TILE, t * TILE + TILE))
        return carry

    lax.fori_loop(lo, hi, one, 0)


def part_copies(a, r, d):
    x = around(a.x, d, NX)
    return (
        remote(r.ob.at[d], r.orc.at[d], r.o_ss.at[d], r.o_rs.at[d], x=x),
        remote(r.lb.at[d], r.lrc.at[d], r.l_ss.at[d], r.l_rs.at[d], x=x),
    )


def mix_last_rows(a, r, d):
    xs = around(a.x, d, NX)
    dst_o, dst_l = (r.ob, r.lb) if d else (r.orc, r.lrc)
    for t in range(2 * ROWS // TILE):
        at = slice(t * TILE, t * TILE + TILE)
        attend_rows(r, xs, at)
        acc = r.acc[xs, at, :]
        total = acc[:, 128:]
        dst_o[d, at, :] = (acc[:, :128] / total).astype(BF16)
        lse = r.mx[xs, at, :] + jnp.log2(total)
        for b in range(TILE // 128):
            row = t * (TILE // 128) + b
            dst_l[d, row : row + 1, :] = to_row(lse[b * 128 : b * 128 + 128, :])
    if d:
        for cp in part_copies(a, r, d):
            cp.start()


def mix_combine(a, r):
    for d in (1, 2, 3):
        for cp in part_copies(a, r, d):
            cp.wait_recv()
    for b in range(6):
        lse = [to_col(r.lrc[d, b : b + 1, :]) for d in range(NX)]
        top = functools.reduce(jnp.maximum, lse)
        w = [jnp.exp2(v - top) for v in lse]
        inv = 1.0 / functools.reduce(jnp.add, w)
        at = slice(b * 128, b * 128 + 128)
        o = None
        for d in range(NX):
            term = r.orc[d, at, :].astype(F32) * (w[d] * inv)
            o = term if o is None else o + term
        h, t = b // 3, b % 3
        r.att[t * 128 : t * 128 + 128, h * 128 : h * 128 + 128] = o.astype(BF16)


def project(r, half):
    for j in range(4):
        off = pl.multiple_of(half * 1024 + j * 256, 256)
        o = jnp.dot(r.att[...], r.wo[:, pl.ds(off, 256)], preferred_element_type=F32)
        r.mp[half, :, j * 256 : j * 256 + 256] = o.astype(BF16)


def mix_pair_copy(a, r):
    return remote(r.mp.at[1 - a.c], r.mr, r.m_ss.at[0], r.m_rs.at[0], c=1 - a.c)


def mix_tree_copy(a, r, role):
    return tree_copy(a, r.ms, r.yl, r.yr, r.y_ss, r.y_rs, role)


def mix_project(a, r):
    pltpu.make_async_copy(r.wo_h, r.wo, r.wo_sem).wait()
    project(r, 1 - a.c)
    mix_pair_copy(a, r).start()
    project(r, a.c)
    mix_pair_copy(a, r).wait_recv()


def mix_pair_total(a, r, i):
    y = around(a.y, PAIR_ORDER[i], NY)
    at = pl.ds(pl.multiple_of(y * 48, 16), 48)
    return y, r.mp[a.c, at, :].astype(F32) + r.mr[at, :].astype(F32)


def mix_scatter(a, r):
    for role in range(5):
        y, total = mix_pair_total(a, r, role)
        r.ms[y] = total.astype(BF16)
        mix_tree_copy(a, r, role).start()
    r.fs[...] = mix_pair_total(a, r, 7)[1]


def mix_relay(a, r):
    mix_tree_copy(a, r, 2).wait_recv()
    for role in (5, 6):
        y, total = mix_pair_total(a, r, role)
        mix_tree_copy(a, r, role - 5).wait_recv()
        r.ms[y] = (total + relayed(a, r.yl, role)).astype(BF16)
        mix_tree_copy(a, r, role).start()


def mix_final_copy(a, r):
    src = r.fs.at[pl.ds(pl.multiple_of((1 - a.c) * 24, 8), 24)]
    return remote(src, r.fr, r.f_ss, r.f_rs, c=1 - a.c)


def mix_sum(a, r):
    total = r.fs[...]
    for role in range(3, 7):
        mix_tree_copy(a, r, role).wait_recv()
        total = total + r.yr[role - 3].astype(F32)
    r.fs[...] = total
    mix_final_copy(a, r).start()


def mix_finish(a, r, out):
    mix_final_copy(a, r).wait()
    mine = r.fs[pl.ds(pl.multiple_of(a.c * 24, 8), 24), :]
    other = r.fr[...]
    sq = jnp.sum(mine * mine, axis=1, keepdims=True) + jnp.sum(other * other, axis=1, keepdims=True)
    inv = lax.rsqrt(sq * (1.0 / D) + EPS)
    for half, v in ((a.c, mine), (1 - a.c, other)):
        off = pl.ds(pl.multiple_of(half * 1024, 1024), 1024)
        out[:, off] = (v * inv * r.mgain[:, off]).astype(BF16)
    for d in (1, 2, 3):
        q_copy(a, r, d).wait_send()
        for cp in part_copies(a, r, d):
            cp.wait_send()
    for slot in range(OWN):
        for cp in kv_copies(a, r, slot):
            cp.wait_send()
    mix_pair_copy(a, r).wait_send()
    for role in range(7):
        mix_tree_copy(a, r, role).wait_send()


def bind(names, refs):
    return SimpleNamespace(**dict(zip(names, refs, strict=True)))


def kernel(*refs):
    r = bind((*MOE_IN[:-3], *MIX_IN[:-1], *MOE_IN[-3:], MIX_IN[-1], "moe_out", "mix_out", *SCRATCH), refs)
    a = here()
    r.drecv[...] = jnp.zeros(r.drecv.shape, BF16)
    r.rrecv[...] = jnp.zeros(r.rrecv.shape, BF16)
    barrier = pltpu.get_barrier_semaphore()
    greet_ep(a, barrier)
    greet_tp(a, barrier)
    moe_weights(r)
    moe_dispatch_build(a, r)
    mix_turn(a, r)
    pl.semaphore_wait(barrier, 46)
    exchange_start(a, r.disp, r.drecv, r.d_ss, r.d_rs)
    mix_send(a, r)
    exchange_wait(r.disp, r.drecv, r.d_ss, r.d_rs)
    moe_compact(a, r)
    moe_gather_start(a, r)
    mix_step(a, r, 0)
    for d in (1, 2, 3):
        q_copy(a, r, d).wait_recv()
    mix_rows(r, 0, 4)
    moe_gather_forward(a, r, 0)
    mix_step(a, r, 1)
    mix_rows(r, 0, 2)
    moe_experts(a, r, 0)
    moe_gather_forward(a, r, 1)
    mix_rows(r, 2, 4)
    moe_pair_sums(a, r, 0)
    mix_step(a, r, 2)
    moe_experts(a, r, 1)
    moe_gather_forward(a, r, 2)
    mix_rows(r, 0, 2)
    moe_pair_sums(a, r, 1)
    moe_experts(a, r, 2)
    moe_relay(a, r, 0)
    mix_rows(r, 2, 4)
    moe_pair_sums(a, r, 2)
    mix_step(a, r, 3)
    mix_last_rows(a, r, 2)
    moe_relay(a, r, 1)
    for d in (1, 3, 0):
        mix_last_rows(a, r, d)
    moe_relay(a, r, 2)
    moe_return_start(a, r)
    mix_combine(a, r)
    mix_project(a, r)
    mix_scatter(a, r)
    moe_combine(a, r)
    mix_relay(a, r)
    mix_sum(a, r)
    moe_finish(a, r, r.moe_out)
    mix_finish(a, r, r.mix_out)


SCRATCH = MOE_SCRATCH | MIX_SCRATCH


def call(ins, hbm):
    n = len(ins) - hbm
    return pl.pallas_call(
        kernel,
        out_shape=(jax.ShapeDtypeStruct((TOKENS2, 128), BF16), jax.ShapeDtypeStruct((24, D), BF16)),
        in_specs=[pl.BlockSpec(memory_space=pltpu.VMEM)] * n + [pl.BlockSpec(memory_space=pl.ANY)] * hbm,
        out_specs=(pl.BlockSpec(memory_space=pltpu.VMEM),) * 2,
        scratch_shapes=list(SCRATCH.values()),
        compiler_params=pltpu.CompilerParams(
            collective_id=0, has_side_effects=True, vmem_limit_bytes=60 * 2**20
        ),
        cost_estimate=pl.CostEstimate(flops=10**10, bytes_accessed=2**23, transcendentals=0),
    )(*ins)


def turn_tables():
    freq = (THETA ** (-np.arange(0, 64, 2, dtype=np.float32) / np.float32(64))).astype(np.float32)
    row = np.arange(192, dtype=np.float32)[:, None] * freq[None]
    col = np.arange(64, dtype=np.float32)[:, None] * freq[None]
    rowcs = np.zeros((2, 192, 128), np.float32)
    colcs = np.zeros((2, 64, 128), np.float32)
    rowcs[0, :, 0:32] = rowcs[0, :, 32:64] = np.cos(row)
    rowcs[1, :, 0:32], rowcs[1, :, 32:64] = -np.sin(row), np.sin(row)
    colcs[0, :, 64:96] = colcs[0, :, 96:128] = np.cos(col)
    colcs[1, :, 64:96], colcs[1, :, 96:128] = -np.sin(col), np.sin(col)
    return jnp.asarray(rowcs), jnp.asarray(colcs)


def per_device(
    query_rows,
    key_rows,
    value_rows,
    query_gain,
    key_gain,
    w_out,
    mixer_gain,
    expert_input,
    expert_ids,
    expert_weights,
    input_gain,
    w_gate,
    w_up,
    w_down,
    out_gain,
):
    rowcs, colcs = turn_tables()
    moe, mix = call(
        (
            expert_input,
            expert_ids.T,
            expert_weights.T,
            input_gain.reshape(1, D),
            out_gain.reshape(1, 128),
            query_rows,
            key_rows,
            value_rows,
            query_gain.reshape(1, HEAD),
            key_gain.reshape(1, HEAD),
            rowcs,
            colcs,
            mixer_gain.reshape(1, D),
            w_gate[0],
            w_up[0],
            w_down[0],
            w_out,
        ),
        4,
    )
    return (mix, moe)


def solution(mesh):
    finer = Mesh(mesh.devices.reshape(NZ, NX, NY, NC), ("z", "x", "y", "c"))
    in_specs = (
        P(EP, TP),
        P(EP, TP),
        P(EP, TP),
        P(),
        P(),
        P(TP, None),
        P(),
        P(EP, None),
        P(EP, None),
        P(EP, None),
        P(),
        P(EP, None, TP),
        P(EP, None, TP),
        P(EP, TP, None),
        P(TP),
    )
    out_specs = (P(EP + TP, None), P(EP, TP))
    return jax.shard_map(
        per_device, mesh=finer, in_specs=in_specs, out_specs=out_specs, check_vma=False
    )
```
